32 devices in a mesh: sp: 8 (over z, x), tp: 4 (over y, core).
Axes of the slice: x: 2, y: 2, z: 4, core: 2. Of those that a mesh axis runs over, the one named last changes fastest.
Arguments:
- latents: bfloat16 [4096, 2048], P(('sp', 'tp')), may hold values from -6 to 6
- context: bfloat16 [512, 2048], P('sp'), may hold values from -6 to 6
- cond: float32 [2048], P('sp'), may hold values from -6 to 6
- ctx_cond: float32 [2048], P('sp'), may hold values from -6 to 6
- mod_weight: float32 [2048, 6144], P('sp', 'tp'), may hold values from -0.125 to 0.125
- query_weight: bfloat16 [2048, 2048], P(None, 'tp'), may hold values from -1 to 1, as said below
- key_matrix: bfloat16 [2048, 1024], P(None, 'tp'), may hold values from -1 to 1, as said below
- value_matrix: bfloat16 [2048, 1024], P(None, 'tp'), may hold values from -0.125 to 0.125
- out_weight: bfloat16 [2048, 2048], P('tp'), may hold values from -0.125 to 0.125
- query_gain: float32 [128], replicated, may hold values from 0.7 to 7
- key_gain: float32 [128], replicated, may hold values from 0.7 to 7
Outputs:
- updated: bfloat16 [4096, 2048], P(('sp', 'tp'))
The draws below stay inside these ranges and needn't reach their ends.
Inputs may be any that keep to these rules, and one draw needn't show every extreme that they name: `query_weight`: entries of order 2048 to the power -1/2. `key_matrix`: entries of order 2048 to the power -1/2.
All inputs are finite; a program needn't handle non-finite values.
Results may differ from the reference program's by a relative error of at most 0.0085.
The reference program's roundings to bfloat16 on the way count: a program that leaves them out, or rounds other values in their place, can miss the bound.
Values may be sent and summed in bfloat16 or wider, within the bound.
A program may use at most 128 MiB of HBM per device.

```python
import math
import jax
import jax.numpy as jnp
from jax import lax

MODEL_DIM = 2048
HEAD_SIZE = 128
QUERY_HEAD_COUNT = 16
KEY_VALUE_HEADS = 8
GRID_W = 64
CTX = 512
TOKENS = 4096


def paired_weights(key):
    query_base = jax.random.normal(jax.random.fold_in(key, 11), (MODEL_DIM, QUERY_HEAD_COUNT * HEAD_SIZE), jnp.float32) * MODEL_DIM ** (-0.5)
    key_start = jax.random.normal(jax.random.fold_in(key, 12), (MODEL_DIM, KEY_VALUE_HEADS * HEAD_SIZE), jnp.float32) * MODEL_DIM ** (-0.5)
    return (query_base, key_start)


def draw_query_weight(key, part):
    return paired_weights(key)[0].astype(jnp.bfloat16)


def draw_key_matrix(key, part):
    return paired_weights(key)[1].astype(jnp.bfloat16)


def draw_query_gain(key, part):
    return jax.random.uniform(jax.random.fold_in(key, 21), (HEAD_SIZE,), jnp.float32, 0.7, 1.3)


def draw_key_gain(key, part):
    return jax.random.uniform(jax.random.fold_in(key, 22), (HEAD_SIZE,), jnp.float32, 0.7, 1.3)


def shard_levels(rng, dims, shards, smallest, high):
    loudness, own = 1.0, jax.random.fold_in(rng, 6)
    for position, parts in shards:
        draws = jnp.exp(jax.random.uniform(jax.random.fold_in(own, position), (parts,), jnp.float32, smallest / len(shards), high / len(shards)))
        loudness = loudness * jnp.repeat(draws, dims[position] // parts).reshape([-1 if axis == position else 1 for axis in range(len(dims))])
    return loudness


def centred(stream_key, dims, width, most, pieces=(), kind=jnp.bfloat16):
    result = jax.random.normal(stream_key, dims, jnp.float32) * width
    if len(pieces) > 0:
        result = shard_levels(stream_key, dims, pieces, -0.22, 0.18) * result
    return jnp.clip(result, min=-most, max=most).astype(kind)


def setup_inputs(seed: int = 0) -> dict:
    key_of = jax.random.split(jax.random.key(seed), 12)
    latents = centred(key_of[0], (TOKENS, MODEL_DIM), 1.0, 6.0, ((0, 32),))
    context = centred(key_of[1], (CTX, MODEL_DIM), 1.0, 6.0, ((0, 8),))
    cond = centred(key_of[2], (MODEL_DIM,), 1.0, 6.0, ((0, 8),), jnp.float32)
    ctx_cond = centred(key_of[3], (MODEL_DIM,), 1.0, 6.0, ((0, 8),), jnp.float32)
    mod_weight = centred(key_of[4], (MODEL_DIM, 3 * MODEL_DIM), MODEL_DIM ** -0.5, 0.125, ((0, 8), (1, 4)), jnp.float32)
    query_weight = draw_query_weight(jax.random.fold_in(key_of[11], 71), 0)
    key_matrix = draw_key_matrix(jax.random.fold_in(key_of[11], 71), 0)
    value_matrix = centred(key_of[7], (MODEL_DIM, KEY_VALUE_HEADS * HEAD_SIZE), MODEL_DIM ** -0.5, 0.125, ((1, 4),))
    out_weight = centred(key_of[8], (QUERY_HEAD_COUNT * HEAD_SIZE, MODEL_DIM), (QUERY_HEAD_COUNT * HEAD_SIZE) ** -0.5, 0.125, ((0, 4),))
    query_gain = draw_query_gain(jax.random.fold_in(key_of[11], 71), 0)
    key_gain = draw_key_gain(jax.random.fold_in(key_of[11], 71), 0)
    return {"latents": latents, "context": context, "cond": cond, "ctx_cond": ctx_cond, "mod_weight": mod_weight, "query_weight": query_weight, "key_matrix": key_matrix, "value_matrix": value_matrix, "out_weight": out_weight, "query_gain": query_gain, "key_gain": key_gain}


NORM_EPS = 1e-06
ROPE_BASE = 10000.0

def normalize(latent_value_rows):
    return latent_value_rows * lax.rsqrt(lax.optimization_barrier(jnp.mean(latent_value_rows * latent_value_rows, axis=-1, keepdims=True)) + NORM_EPS)

def rotate(latent_value_rows, positions):
    quarter = latent_value_rows.shape[-1] // 2
    inv_freq = ROPE_BASE ** (-jnp.arange(quarter, dtype=jnp.float32) / quarter)
    angles = positions.astype(jnp.float32)[:, None] * inv_freq[None, :]
    cos_table = jnp.cos(angles)[:, None, :]
    sin_table = jnp.sin(angles)[:, None, :]
    first, second = (latent_value_rows[..., :quarter], latent_value_rows[..., quarter:])
    return jnp.concatenate([first * cos_table - second * sin_table, second * cos_table + first * sin_table], axis=-1)

def axial(latent_value_rows, positions):
    half_dim = latent_value_rows.shape[-1] // 2
    return jnp.concatenate([rotate(latent_value_rows[..., :half_dim], positions // GRID_W), rotate(latent_value_rows[..., half_dim:], positions % GRID_W)], axis=-1)

def modulate(latent_value_rows, mod_row):
    model_width = latent_value_rows.shape[-1]
    shift_vec = mod_row[:model_width]
    scale_vec = mod_row[model_width:2 * model_width]
    return (normalize(latent_value_rows.astype(jnp.float32)) * (1.0 + scale_vec) + shift_vec).astype(jnp.bfloat16)

def reference(latents, context, cond, ctx_cond, mod_weight, query_weight, key_matrix, value_matrix, out_weight, query_gain, key_gain):
    model_width = latents.shape[1]
    latent_count = latents.shape[0]
    prefix_count = context.shape[0]
    modulation = jnp.dot(jax.nn.silu(jnp.stack([cond, ctx_cond])), mod_weight, precision=lax.Precision.HIGHEST)
    gate_vec = modulation[0, 2 * model_width:]
    normalised_rows = modulate(latents, modulation[0])
    prefix_normalised = modulate(context, modulation[1])
    positions = jnp.arange(latent_count, dtype=jnp.int32)
    query_rows = jnp.dot(normalised_rows, query_weight, preferred_element_type=jnp.float32).reshape(latent_count, QUERY_HEAD_COUNT, HEAD_SIZE)
    query_rows = axial(normalize(query_rows) * query_gain, positions).astype(jnp.bfloat16)
    latent_key_rows = jnp.dot(normalised_rows, key_matrix, preferred_element_type=jnp.float32).reshape(latent_count, KEY_VALUE_HEADS, HEAD_SIZE)
    latent_key_rows = axial(normalize(latent_key_rows) * key_gain, positions).astype(jnp.bfloat16)
    latent_value_rows = jnp.dot(normalised_rows, value_matrix, preferred_element_type=jnp.float32).reshape(latent_count, KEY_VALUE_HEADS, HEAD_SIZE).astype(jnp.bfloat16)
    prefix_keys = jnp.dot(prefix_normalised, key_matrix, preferred_element_type=jnp.float32).reshape(prefix_count, KEY_VALUE_HEADS, HEAD_SIZE)
    prefix_keys = (normalize(prefix_keys) * key_gain).astype(jnp.bfloat16)
    prefix_values = jnp.dot(prefix_normalised, value_matrix, preferred_element_type=jnp.float32).reshape(prefix_count, KEY_VALUE_HEADS, HEAD_SIZE).astype(jnp.bfloat16)
    keys_all = jnp.concatenate([prefix_keys, latent_key_rows], axis=0).astype(jnp.float32)
    values_all = jnp.concatenate([prefix_values, latent_value_rows], axis=0).astype(jnp.float32)
    lift = math.log(latent_count / (2.0 * prefix_count))
    lift_row = jnp.concatenate([jnp.full((prefix_count,), lift, jnp.float32), jnp.zeros((latent_count,), jnp.float32)])
    group_size = QUERY_HEAD_COUNT // KEY_VALUE_HEADS
    rows_per_block = math.gcd(latent_count, 256)
    token_blocks = query_rows.reshape(latent_count // rows_per_block, rows_per_block, KEY_VALUE_HEADS, group_size, HEAD_SIZE)
    inv_root = HEAD_SIZE ** (-0.5)

    def one_block(block):
        scores = jnp.einsum('qhgd,khd->hgqk', block.astype(jnp.float32), keys_all) * inv_root + lift_row
        top_row = lax.optimization_barrier(jnp.max(scores, axis=-1, keepdims=True))
        weights = jnp.exp(scores - top_row)
        total = lax.optimization_barrier(jnp.sum(weights, axis=-1))
        probs = lax.optimization_barrier(weights.astype(jnp.bfloat16)).astype(jnp.float32)
        summed = jnp.einsum('hgqk,khd->qhgd', probs, values_all)
        return (summed / jnp.transpose(total, (2, 0, 1))[..., None]).astype(jnp.bfloat16)
    attended = lax.map(one_block, token_blocks).reshape(latent_count, QUERY_HEAD_COUNT * HEAD_SIZE)
    mixed = jnp.dot(attended, out_weight, preferred_element_type=jnp.float32)
    return (latents.astype(jnp.float32) + gate_vec * normalize(mixed)).astype(jnp.bfloat16)
```

```python
import functools
import math

import jax
import jax.numpy as jnp
from jax import lax
from jax.experimental import pallas as pl
from jax.experimental.pallas import tpu as pltpu
from jax.sharding import PartitionSpec as P

GRID_W = 64
NORM_EPS = 1e-06
ROPE_BASE = 10000.0
MESH = pl.DeviceIdType.MESH
BF16 = jnp.bfloat16
F32 = jnp.float32


def row_size(sp_count):
    size = 1
    while 4 * size * size <= sp_count:
        size *= 2
    return size


def tables(positions, head_dim):
    quarter = head_dim // 4
    inv_freq = ROPE_BASE ** (-jnp.arange(quarter, dtype=F32) / quarter)
    row_ang = inv_freq[:, None] * (positions // GRID_W).astype(F32)[None, :]
    col_ang = inv_freq[:, None] * (positions % GRID_W).astype(F32)[None, :]
    cos = jnp.concatenate([jnp.cos(row_ang)] * 2 + [jnp.cos(col_ang)] * 2, axis=0)
    row_sin, col_sin = jnp.sin(row_ang), jnp.sin(col_ang)
    sin = jnp.concatenate([-row_sin, row_sin, -col_sin, col_sin], axis=0)
    return cos, sin


def remote(src, dst, send, recv, dev):
    return pltpu.make_async_remote_copy(
        src_ref=src, dst_ref=dst, send_sem=send, recv_sem=recv, device_id=dev, device_id_type=MESH
    )


def front_kernel(
    sp_count, tp_count, head_dim,
    cond_ref, mw_hbm, lat_hbm, ctx_ref, wq_hbm, wk_hbm, wv_hbm, qg_ref, kg_ref, cos_ref, sin_ref,
    qt_ref, k_ref, vt_ref, ck_ref, cv_ref, gate_ref,
    mw, lat, wq, wk, wv, part, tot, mod, xn, load_sem,
    lat_send, lat_recv, part_send, part_recv, tot_send, tot_recv,
):
    s, t = lax.axis_index("sp"), lax.axis_index("tp")
    y, c = t // 2, t % 2
    y_count = tp_count // 2
    partner = y * 2 + 1 - c
    rows = lat.shape[1]
    width = lat.shape[2]
    model_cols = mod.shape[1]

    own = pltpu.make_async_copy(lat_hbm, lat.at[t], load_sem.at[0])
    own.start()
    loads = [
        pltpu.make_async_copy(a, b, load_sem.at[1 + i])
        for i, (a, b) in enumerate(((mw_hbm, mw), (wq_hbm, wq), (wk_hbm, wk), (wv_hbm, wv)))
    ]
    for one in loads:
        one.start()

    barrier = pltpu.get_barrier_semaphore()
    for j in range(1, sp_count):
        pl.semaphore_signal(barrier, inc=1, device_id=((s + j) % sp_count, t), device_id_type=MESH)
    for j in range(1, tp_count):
        pl.semaphore_signal(barrier, inc=1, device_id=(s, (t + j) % tp_count), device_id_type=MESH)
    pl.semaphore_wait(barrier, sp_count + tp_count - 2)

    own.wait()
    sends = []
    for j in range(1, y_count):
        peer = ((y + j) % y_count) * 2 + c
        sends.append(remote(lat.at[t], lat.at[t], lat_send.at[j], lat_recv.at[t], (s, peer)))
    sends.append(remote(lat.at[t], lat.at[t], lat_send.at[0], lat_recv.at[t], (s, partner)))
    for one in sends:
        one.start()

    loads[0].wait()
    cond = cond_ref[...]
    cond = cond * jax.nn.sigmoid(cond)
    part[s] = jnp.dot(
        cond, mw[...], precision=lax.Precision.HIGHEST, preferred_element_type=F32
    )[:2]
    more = [
        remote(part.at[s], part.at[s], part_send.at[j], part_recv.at[s], ((s + j) % sp_count, t))
        for j in range(1, sp_count)
    ]
    for one in more:
        one.start()
    for j in range(1, sp_count):
        src = (s + j) % sp_count
        remote(part.at[src], part.at[src], part_send.at[0], part_recv.at[src], (s, t)).wait_recv()
    total = part[0]
    for j in range(1, sp_count):
        total = total + part[j]
    tot[t] = total
    last = [
        remote(tot.at[t], tot.at[t], tot_send.at[j], tot_recv.at[t], (s, (t + j) % tp_count))
        for j in range(1, tp_count)
    ]
    for one in last:
        one.start()
    for j in range(1, tp_count):
        src = (t + j) % tp_count
        remote(tot.at[src], tot.at[src], tot_send.at[0], tot_recv.at[src], (s, t)).wait_recv()
    cols = model_cols // tp_count
    for j in range(tp_count):
        mod[:, j * cols : (j + 1) * cols] = tot[j]
    gate_ref[...] = mod[0:1, 2 * width :]

    def modulate(x, r):
        x = x.astype(F32)
        scaled = x * lax.rsqrt(jnp.mean(x * x, axis=-1, keepdims=True) + NORM_EPS)
        shift, scale = mod[r : r + 1, :width], mod[r : r + 1, width : 2 * width]
        return (scaled * (1.0 + scale) + shift).astype(BF16)

    for one in loads[1:]:
        one.wait()

    cn = modulate(ctx_ref[...], 1)
    kc = jnp.dot(cn, wk[...], preferred_element_type=F32)
    vc = jnp.dot(cn, wv[...], preferred_element_type=F32)
    for h in range(kc.shape[1] // head_dim):
        kh = kc[:, h * head_dim : (h + 1) * head_dim]
        kh = kh * lax.rsqrt(jnp.mean(kh * kh, axis=-1, keepdims=True) + NORM_EPS) * kg_ref[...]
        ck_ref[h] = kh.astype(BF16)
        cv_ref[h] = vc[:, h * head_dim : (h + 1) * head_dim].astype(BF16)

    q4 = head_dim // 4
    qgain, kgain = qg_ref[...], kg_ref[...]

    def turn(yt, cos, sin):
        part_t = jnp.concatenate(
            [yt[q4 : 2 * q4], yt[:q4], yt[3 * q4 :], yt[2 * q4 : 3 * q4]], axis=0
        )
        return yt * cos + part_t * sin

    def unit(yh, gain):
        return yh * lax.rsqrt(jnp.mean(yh * yh, axis=-1, keepdims=True) + NORM_EPS) * gain

    span = 2 * rows
    relays = []
    for j in range(y_count):
        yy = (y + j) % y_count
        if j > 0:
            src = yy * 2 + c
            remote(lat.at[src], lat.at[src], lat_send.at[0], lat_recv.at[src], (s, t)).wait_recv()
            one = remote(
                lat.at[src], lat.at[src], lat_send.at[y_count - 1 + j], lat_recv.at[src], (s, partner)
            )
            one.start()
            relays.append(one)
        other = yy * 2 + 1 - c
        remote(lat.at[other], lat.at[other], lat_send.at[0], lat_recv.at[other], (s, t)).wait_recv()
        for i in range(2):
            xn[i * rows : (i + 1) * rows, :] = modulate(lat[yy * 2 + i], 0)
        x = xn[...]
        at = pl.ds(pl.multiple_of(yy * span, span), span)
        cos, sin = cos_ref[:, at], sin_ref[:, at]
        for w, kind in ((wq, 0), (wk, 1), (wv, 2)):
            step = min(2 * head_dim, w.shape[1])
            for n in range(0, w.shape[1], step):
                full = jnp.dot(x, w[:, n : n + step], preferred_element_type=F32)
                for m in range(0, step, head_dim):
                    h = (n + m) // head_dim
                    yh = full[:, m : m + head_dim]
                    if kind == 0:
                        qt_ref[h, :, at] = turn(unit(yh, qgain).T, cos, sin).astype(BF16)
                    elif kind == 1:
                        k_ref[h, at, :] = turn(unit(yh, kgain).T, cos, sin).T.astype(BF16)
                    else:
                        vt_ref[h, :, at] = yh.T.astype(BF16)
    for one in sends + more + last + relays:
        one.wait_send()


def attend_kernel(
    sp_count, x_count, group, lift,
    k_hbm, vt_hbm, ck_hbm, cv_hbm, qt_ref,
    out_ref,
    kb, vb, cb, top, tot, acc, load_sem, send_sem, recv_sem,
):
    s, t = lax.axis_index("sp"), lax.axis_index("tp")
    z, x = s // x_count, s % x_count
    z_count = sp_count // x_count
    heads, head_dim, rows = qt_ref.shape
    kv_heads = heads // group
    factor = head_dim ** (-0.5) * math.log2(math.e)

    loads = [
        pltpu.make_async_copy(a, b, load_sem.at[i])
        for i, (a, b) in enumerate(
            (
                (ck_hbm, cb.at[s, 0]),
                (cv_hbm, cb.at[s, 1]),
                (k_hbm, kb.at[s]),
                (vt_hbm, vb.at[s]),
            )
        )
    ]
    for one in loads:
        one.start()
    barrier = pltpu.get_barrier_semaphore()
    targets = []
    for sign in (1, -1):
        ok = (z + sign >= 0) & (z + sign < z_count)
        peer = ((z + sign + z_count) % z_count) * x_count + x
        targets.append((ok, peer))
    for ok, peer in targets:

        @pl.when(ok)
        def _():
            pl.semaphore_signal(barrier, inc=1, device_id=(peer, t), device_id_type=MESH)

    for j in range(1, x_count):
        peer = z * x_count + (x + j) % x_count
        pl.semaphore_signal(barrier, inc=1, device_id=(peer, t), device_id_type=MESH)
    ends_here = (z == 0).astype(jnp.int32) + (z == z_count - 1).astype(jnp.int32)
    pl.semaphore_wait(barrier, x_count + 1 - ends_here)

    top[...] = jnp.full_like(top, -1e30)
    tot[...] = jnp.zeros_like(tot)
    acc[...] = jnp.zeros_like(acc)
    for one in loads:
        one.wait()

    bufs = (cb, kb, vb)

    def copies(src, way, peer):
        return [
            remote(b.at[src], b.at[src], send_sem.at[i, src, way], recv_sem.at[i, src], (peer, t))
            for i, b in enumerate(bufs)
        ]

    def source(k):
        low = jnp.minimum(z, z_count - 1 - z)
        both = k <= 2 * low
        dist = jnp.where(both, (k + 1) // 2, k - low)
        up = jnp.where(both, k % 2 == 1, z < z_count - 1 - z)
        return jnp.where(up, z + dist, z - dist)

    def update(i, keys, values_t, bias):
        sc = jnp.dot(keys, qt_ref[i], preferred_element_type=F32) * factor
        if bias != 0.0:
            sc = sc + bias
        old = top[i]
        new = jnp.maximum(old, jnp.max(sc, axis=0, keepdims=True))
        p = jnp.exp2(sc - new)
        f = jnp.exp2(old - new)
        top[i] = new
        tot[i] = tot[i] * f + jnp.sum(p, axis=0, keepdims=True)
        acc[i] = acc[i] * f + jnp.dot(values_t, p.astype(BF16), preferred_element_type=F32)

    def block(src):
        def head(i, carry):
            h = i // group
            update(i, kb[src, h], vb[src, h], 0.0)
            return carry

        lax.fori_loop(0, heads, head, 0)

    def wait_from(src):
        for one in copies(src, 0, s):
            one.wait_recv()

    def step(k, carry):
        zz = source(k)
        src = zz * x_count + x

        @pl.when(k > 0)
        def _():
            wait_from(src)

        for way, (ok, peer) in enumerate(targets):
            mine = zz <= z if way == 0 else zz >= z

            @pl.when(ok & mine)
            def _():
                for one in copies(src, way, peer):
                    one.start()

        for j in range(1, x_count):
            for one in copies(src, 1 + j, z * x_count + (x + j) % x_count):
                one.start()
        block(src)

        @pl.when(k > 0)
        def _():
            before = source(k - 1)
            for j in range(1, x_count):
                old = before * x_count + (x + j) % x_count
                wait_from(old)
                block(old)

        return carry

    lax.fori_loop(0, z_count, step, 0)
    final = source(z_count - 1)
    ends = [final * x_count + (x + j) % x_count for j in range(1, x_count)]
    for src in ends:
        copies(src, 0, s)[0].wait_recv()
    for i in range(heads):
        h = i // group
        keys = jnp.concatenate([cb[j, 0, h] for j in range(sp_count)], axis=0)
        vals = jnp.concatenate([cb[j, 1, h] for j in range(sp_count)], axis=0)
        update(i, keys, vals.astype(F32).T.astype(BF16), lift * math.log2(math.e))
    for src in ends:
        for one in copies(src, 0, s)[1:]:
            one.wait_recv()
        block(src)
    for i in range(heads):
        out_ref[:, i * head_dim : (i + 1) * head_dim] = (acc[i] / tot[i]).T.astype(BF16)

    def drain(k, carry):
        zz = source(k)
        src = zz * x_count + x
        for way, (ok, peer) in enumerate(targets):
            mine = zz <= z if way == 0 else zz >= z

            @pl.when(ok & mine)
            def _():
                for one in copies(src, way, peer):
                    one.wait_send()

        for j in range(1, x_count):
            for one in copies(src, 1 + j, z * x_count + (x + j) % x_count):
                one.wait_send()
        return carry

    lax.fori_loop(0, z_count, drain, 0)


def mix_kernel(
    tp_count, chunks,
    att_ref, wo_ref, lat_ref, gate_ref,
    out_ref,
    core_out, core_in, mesh_out, mesh_in, mixed, core_send, core_recv, mesh_send, mesh_recv,
):
    s, t = lax.axis_index("sp"), lax.axis_index("tp")
    y, c = t // 2, t % 2
    y_count = tp_count // 2
    partner = y * 2 + 1 - c
    rows, width = lat_ref.shape
    step = width // chunks
    barrier = pltpu.get_barrier_semaphore()
    peers = [((y + j) % y_count) * 2 + c for j in range(1, y_count)]
    for peer in peers + [partner]:
        pl.semaphore_signal(barrier, inc=1, device_id=(s, peer), device_id_type=MESH)
    pl.semaphore_wait(barrier, y_count)

    def piece(n, j, cc):
        yy = (y + j) % y_count
        at = pl.ds(pl.multiple_of((yy * 2 + cc) * rows, rows), rows)
        return jnp.dot(
            att_ref[at, :], wo_ref[:, n * step : (n + 1) * step], preferred_element_type=F32
        )

    order = list(range(1, y_count)) + [0]
    cores = [
        remote(core_out.at[n], core_in.at[n], core_send.at[n], core_recv.at[n], (s, partner))
        for n in range(chunks)
    ]
    sent = []
    for n in range(chunks):
        for j in order:
            core_out[n, j] = piece(n, j, 1 - c).astype(BF16)
        cores[n].start()
    for n in range(chunks):
        mine = [piece(n, j, c) for j in order]
        cores[n].wait_recv()
        for j, value in zip(order, mine):
            value = value + core_in[n, j].astype(F32)
            if j == 0:
                mixed[n] = value
            else:
                mesh_out[n, j - 1] = value.astype(BF16)
                one = remote(
                    mesh_out.at[n, j - 1], mesh_in.at[n, j - 1], mesh_send.at[n, j - 1],
                    mesh_recv.at[n, j - 1], (s, peers[j - 1]),
                )
                one.start()
                sent.append(one)
    for one in sent:
        one.wait_recv()
    square = jnp.zeros((rows, 1), F32)
    for n in range(chunks):
        value = mixed[n]
        for j in range(1, y_count):
            value = value + mesh_in[n, j - 1].astype(F32)
        mixed[n] = value
        square = square + jnp.sum(value * value, axis=-1, keepdims=True)
    inv = lax.rsqrt(square / width + NORM_EPS)
    for n in range(chunks):
        at = slice(n * step, (n + 1) * step)
        out_ref[:, at] = (
            lat_ref[:, at].astype(F32) + gate_ref[:, at] * (mixed[n] * inv)
        ).astype(BF16)
    for one in sent + cores:
        one.wait_send()


ANY = pl.BlockSpec(memory_space=pl.ANY)
VM = pl.BlockSpec(memory_space=pltpu.VMEM)
DMA = pltpu.SemaphoreType.DMA


def body(
    latents,
    context,
    cond,
    ctx_cond,
    mod_weight,
    query_weight,
    key_matrix,
    value_matrix,
    out_weight,
    query_gain,
    key_gain,
):
    sp_count, tp_count = lax.axis_size("sp"), lax.axis_size("tp")
    x_count = row_size(sp_count)
    rows, width = latents.shape
    ctx_rows = context.shape[0]
    head_dim = query_gain.shape[0]
    heads = query_weight.shape[1] // head_dim
    kv_heads = key_matrix.shape[1] // head_dim
    all_rows = rows * tp_count
    mod_cols = mod_weight.shape[1]
    positions = lax.axis_index("sp") * all_rows + jnp.arange(all_rows, dtype=jnp.int32)
    cos, sin = tables(positions, head_dim)
    pair = jnp.concatenate(
        [cond[None], ctx_cond[None], jnp.zeros((6, cond.shape[0]), F32)], axis=0
    )
    sds = jax.ShapeDtypeStruct
    qt, k, vt, ck, cv, gate = pl.pallas_call(
        functools.partial(front_kernel, sp_count, tp_count, head_dim),
        out_shape=[
            sds((heads, head_dim, all_rows), BF16),
            sds((kv_heads, all_rows, head_dim), BF16),
            sds((kv_heads, head_dim, all_rows), BF16),
            sds((kv_heads, ctx_rows, head_dim), BF16),
            sds((kv_heads, ctx_rows, head_dim), BF16),
            sds((1, width), F32),
        ],
        in_specs=[VM, ANY, ANY, VM, ANY, ANY, ANY, VM, VM, VM, VM],
        out_specs=[VM] * 6,
        scratch_shapes=[
            pltpu.VMEM(mod_weight.shape, F32),
            pltpu.VMEM((tp_count, rows, width), BF16),
            pltpu.VMEM(query_weight.shape, BF16),
            pltpu.VMEM(key_matrix.shape, BF16),
            pltpu.VMEM(value_matrix.shape, BF16),
            pltpu.VMEM((sp_count, 2, mod_cols), F32),
            pltpu.VMEM((tp_count, 2, mod_cols), F32),
            pltpu.VMEM((2, mod_cols * tp_count), F32),
            pltpu.VMEM((2 * rows, width), BF16),
            DMA((5,)),
            DMA((tp_count,)),
            DMA((tp_count,)),
            DMA((sp_count,)),
            DMA((sp_count,)),
            DMA((tp_count,)),
            DMA((tp_count,)),
        ],
        compiler_params=pltpu.CompilerParams(
            collective_id=0, has_side_effects=True, vmem_limit_bytes=48 << 20
        ),
        name="front",
    )(
        pair, mod_weight, latents, context, query_weight, key_matrix, value_matrix,
        query_gain[None], key_gain[None], cos, sin,
    )

    lift = math.log(sp_count * all_rows / (2.0 * sp_count * ctx_rows))
    att = pl.pallas_call(
        functools.partial(attend_kernel, sp_count, x_count, heads // kv_heads, lift),
        out_shape=sds((all_rows, heads * head_dim), BF16),
        in_specs=[ANY, ANY, ANY, ANY, VM],
        out_specs=VM,
        scratch_shapes=[
            pltpu.VMEM((sp_count, kv_heads, all_rows, head_dim), BF16),
            pltpu.VMEM((sp_count, kv_heads, head_dim, all_rows), BF16),
            pltpu.VMEM((sp_count, 2, kv_heads, ctx_rows, head_dim), BF16),
            pltpu.VMEM((heads, 1, all_rows), F32),
            pltpu.VMEM((heads, 1, all_rows), F32),
            pltpu.VMEM((heads, head_dim, all_rows), F32),
            DMA((4,)),
            DMA((3, sp_count, x_count + 1)),
            DMA((3, sp_count)),
        ],
        compiler_params=pltpu.CompilerParams(
            collective_id=1, has_side_effects=True, vmem_limit_bytes=48 << 20
        ),
        name="attend",
    )(k, vt, ck, cv, qt)

    chunks = 4
    y_count = tp_count // 2
    step = width // chunks
    far = max(y_count - 1, 1)
    return pl.pallas_call(
        functools.partial(mix_kernel, tp_count, chunks),
        out_shape=sds((rows, width), BF16),
        in_specs=[VM] * 4,
        out_specs=VM,
        scratch_shapes=[
            pltpu.VMEM((chunks, y_count, rows, step), BF16),
            pltpu.VMEM((chunks, y_count, rows, step), BF16),
            pltpu.VMEM((chunks, far, rows, step), BF16),
            pltpu.VMEM((chunks, far, rows, step), BF16),
            pltpu.VMEM((chunks, rows, step), F32),
            DMA((chunks,)),
            DMA((chunks,)),
            DMA((chunks, far)),
            DMA((chunks, far)),
        ],
        compiler_params=pltpu.CompilerParams(
            collective_id=2, has_side_effects=True, vmem_limit_bytes=48 << 20
        ),
        name="mix",
    )(att, out_weight, latents, gate)


def solution(mesh):
    placed = (
        P(("sp", "tp"), None),
        P("sp", None),
        P("sp"),
        P("sp"),
        P("sp", "tp"),
        P(None, "tp"),
        P(None, "tp"),
        P(None, "tp"),
        P("tp", None),
        P(),
        P(),
    )
    return jax.shard_map(
        body, mesh=mesh, in_specs=placed, out_specs=P(("sp", "tp"), None), check_vma=False
    )
```

```python
import functools
import math

import jax
import jax.numpy as jnp
from jax import lax
from jax.experimental import pallas as pl
from jax.experimental.pallas import tpu as pltpu
from jax.sharding import PartitionSpec as P

GRID_W = 64
NORM_EPS = 1e-06
ROPE_BASE = 10000.0
MESH = pl.DeviceIdType.MESH
BF16 = jnp.bfloat16
F32 = jnp.float32
VMEM_BYTES = 67043328


def row_size(sp_count):
    size = 1
    while 4 * size * size <= sp_count:
        size *= 2
    return size


def tables(positions, head_dim):
    quarter = head_dim // 4
    inv_freq = ROPE_BASE ** (-jnp.arange(quarter, dtype=F32) / quarter)
    row_ang = inv_freq[:, None] * (positions // GRID_W).astype(F32)[None, :]
    col_ang = inv_freq[:, None] * (positions % GRID_W).astype(F32)[None, :]
    cos = jnp.concatenate([jnp.cos(row_ang)] * 2 + [jnp.cos(col_ang)] * 2, axis=0)
    row_sin, col_sin = jnp.sin(row_ang), jnp.sin(col_ang)
    sin = jnp.concatenate([-row_sin, row_sin, -col_sin, col_sin], axis=0)
    return cos, sin


def remote(src, dst, send, recv, dev):
    return pltpu.make_async_remote_copy(
        src_ref=src, dst_ref=dst, send_sem=send, recv_sem=recv, device_id=dev, device_id_type=MESH
    )


def front_kernel(
    sp_count, tp_count, head_dim,
    cond_ref, mw_hbm, lat_hbm, ctx_ref, wq_hbm, wk_hbm, wv_hbm, qg_ref, kg_ref, cos_ref, sin_ref,
    qt_ref, k_ref, vt_ref, ckv_ref, gate_ref,
    mw, lat, wq, wk, wv, part, tot, mod, xn, load_sem,
    lat_send, lat_recv, part_send, part_recv, tot_send, tot_recv,
):
    s, t = lax.axis_index("sp"), lax.axis_index("tp")
    y, c = t // 2, t % 2
    y_count = tp_count // 2
    partner = y * 2 + 1 - c
    rows = lat.shape[1]
    width = lat.shape[2]
    model_cols = mod.shape[1]

    own = pltpu.make_async_copy(lat_hbm, lat.at[t], load_sem.at[0])
    own.start()
    loads = [
        pltpu.make_async_copy(a, b, load_sem.at[1 + i])
        for i, (a, b) in enumerate(((mw_hbm, mw), (wq_hbm, wq), (wk_hbm, wk), (wv_hbm, wv)))
    ]
    for one in loads:
        one.start()

    barrier = pltpu.get_barrier_semaphore()
    for j in range(1, sp_count):
        pl.semaphore_signal(barrier, inc=1, device_id=((s + j) % sp_count, t), device_id_type=MESH)
    for j in range(1, tp_count):
        pl.semaphore_signal(barrier, inc=1, device_id=(s, (t + j) % tp_count), device_id_type=MESH)
    pl.semaphore_wait(barrier, sp_count + tp_count - 2)

    own.wait()
    sends = []
    for j in range(1, y_count):
        peer = ((y + j) % y_count) * 2 + c
        sends.append(remote(lat.at[t], lat.at[t], lat_send.at[j], lat_recv.at[t], (s, peer)))
    sends.append(remote(lat.at[t], lat.at[t], lat_send.at[0], lat_recv.at[t], (s, partner)))
    for one in sends:
        one.start()

    loads[0].wait()
    cond = cond_ref[...]
    cond = cond * jax.nn.sigmoid(cond)
    part[s] = jnp.dot(
        cond, mw[...], precision=lax.Precision.HIGHEST, preferred_element_type=F32
    )[:2]
    more = [
        remote(part.at[s], part.at[s], part_send.at[j], part_recv.at[s], ((s + j) % sp_count, t))
        for j in range(1, sp_count)
    ]
    for one in more:
        one.start()
    for j in range(1, sp_count):
        src = (s + j) % sp_count
        remote(part.at[src], part.at[src], part_send.at[0], part_recv.at[src], (s, t)).wait_recv()
    total = part[0]
    for j in range(1, sp_count):
        total = total + part[j]
    tot[t] = total
    last = [
        remote(tot.at[t], tot.at[t], tot_send.at[j], tot_recv.at[t], (s, (t + j) % tp_count))
        for j in range(1, tp_count)
    ]
    for one in last:
        one.start()
    for j in range(1, tp_count):
        src = (t + j) % tp_count
        remote(tot.at[src], tot.at[src], tot_send.at[0], tot_recv.at[src], (s, t)).wait_recv()
    cols = model_cols // tp_count
    for j in range(tp_count):
        mod[:, j * cols : (j + 1) * cols] = tot[j]
    gate_ref[...] = mod[0:1, 2 * width :]

    def modulate(x, r):
        x = x.astype(F32)
        scaled = x * lax.rsqrt(jnp.mean(x * x, axis=-1, keepdims=True) + NORM_EPS)
        shift, scale = mod[r : r + 1, :width], mod[r : r + 1, width : 2 * width]
        return (scaled * (1.0 + scale) + shift).astype(BF16)

    for one in loads[1:]:
        one.wait()

    cn = modulate(ctx_ref[...], 1)
    kc = jnp.dot(cn, wk[...], preferred_element_type=F32)
    vc = jnp.dot(cn, wv[...], preferred_element_type=F32)
    for h in range(kc.shape[1] // head_dim):
        kh = kc[:, h * head_dim : (h + 1) * head_dim]
        kh = kh * lax.rsqrt(jnp.mean(kh * kh, axis=-1, keepdims=True) + NORM_EPS) * kg_ref[...]
        ckv_ref[h, 0] = kh.astype(BF16)
        ckv_ref[h, 1] = vc[:, h * head_dim : (h + 1) * head_dim].astype(BF16)

    q4 = head_dim // 4
    qgain, kgain = qg_ref[...], kg_ref[...]

    def turn(yt, cos, sin):
        part_t = jnp.concatenate(
            [yt[q4 : 2 * q4], yt[:q4], yt[3 * q4 :], yt[2 * q4 : 3 * q4]], axis=0
        )
        return yt * cos + part_t * sin

    def unit(yh, gain):
        return yh * lax.rsqrt(jnp.mean(yh * yh, axis=-1, keepdims=True) + NORM_EPS) * gain

    span = 2 * rows
    relays = []
    for j in range(y_count):
        yy = (y + j) % y_count
        if j > 0:
            src = yy * 2 + c
            remote(lat.at[src], lat.at[src], lat_send.at[0], lat_recv.at[src], (s, t)).wait_recv()
            one = remote(
                lat.at[src], lat.at[src], lat_send.at[y_count - 1 + j], lat_recv.at[src], (s, partner)
            )
            one.start()
            relays.append(one)
        other = yy * 2 + 1 - c
        remote(lat.at[other], lat.at[other], lat_send.at[0], lat_recv.at[other], (s, t)).wait_recv()
        for i in range(2):
            xn[i * rows : (i + 1) * rows, :] = modulate(lat[yy * 2 + i], 0)
        x = xn[...]
        at = pl.ds(pl.multiple_of(yy * span, span), span)
        cos, sin = cos_ref[:, at], sin_ref[:, at]
        for w, kind in ((wq, 0), (wk, 1), (wv, 2)):
            step = min(2 * head_dim, w.shape[1])
            for n in range(0, w.shape[1], step):
                full = jnp.dot(x, w[:, n : n + step], preferred_element_type=F32)
                for m in range(0, step, head_dim):
                    h = (n + m) // head_dim
                    yh = full[:, m : m + head_dim]
                    if kind == 0:
                        qt_ref[h, :, at] = turn(unit(yh, qgain).T, cos, sin).astype(BF16)
                    elif kind == 1:
                        k_ref[h, at, :] = turn(unit(yh, kgain).T, cos, sin).T.astype(BF16)
                    else:
                        vt_ref[h, :, at] = yh.T.astype(BF16)
    for one in sends + more + last + relays:
        one.wait_send()


def attend_kernel(
    sp_count, x_count, group, lift,
    k_hbm, vt_hbm, ckv_hbm, qt_ref,
    out_ref,
    kb, vb, cb, top, tot, acc, load_sem, send_sem, recv_sem,
):
    s, t = lax.axis_index("sp"), lax.axis_index("tp")
    z, x = s // x_count, s % x_count
    z_count = sp_count // x_count
    heads, head_dim, rows = qt_ref.shape
    kv_heads = heads // group
    factor = head_dim ** (-0.5) * math.log2(math.e)

    loads = [
        pltpu.make_async_copy(a, b, load_sem.at[i])
        for i, (a, b) in enumerate(
            (
                (ckv_hbm, cb.at[s]),
                (k_hbm, kb.at[s]),
                (vt_hbm, vb.at[s]),
            )
        )
    ]
    for one in loads:
        one.start()
    barrier = pltpu.get_barrier_semaphore()
    targets = []
    for sign in (1, -1):
        ok = (z + sign >= 0) & (z + sign < z_count)
        peer = ((z + sign + z_count) % z_count) * x_count + x
        targets.append((ok, peer))
    for ok, peer in targets:

        @pl.when(ok)
        def _():
            pl.semaphore_signal(barrier, inc=1, device_id=(peer, t), device_id_type=MESH)

    for j in range(1, x_count):
        peer = z * x_count + (x + j) % x_count
        pl.semaphore_signal(barrier, inc=1, device_id=(peer, t), device_id_type=MESH)
    ends_here = (z == 0).astype(jnp.int32) + (z == z_count - 1).astype(jnp.int32)
    pl.semaphore_wait(barrier, x_count + 1 - ends_here)

    top[...] = jnp.full_like(top, -1e30)
    tot[...] = jnp.zeros_like(tot)
    acc[...] = jnp.zeros_like(acc)
    for one in loads:
        one.wait()

    bufs = (cb, kb, vb)

    def copies(src, way, peer):
        return [
            remote(b.at[src], b.at[src], send_sem.at[i, src, way], recv_sem.at[i, src], (peer, t))
            for i, b in enumerate(bufs)
        ]

    def source(k):
        low = jnp.minimum(z, z_count - 1 - z)
        both = k <= 2 * low
        dist = jnp.where(both, (k + 1) // 2, k - low)
        up = jnp.where(both, k % 2 == 1, z < z_count - 1 - z)
        return jnp.where(up, z + dist, z - dist)

    def update(i, keys, values_t, bias):
        sc = jnp.dot(keys, qt_ref[i], preferred_element_type=F32) * factor
        if bias != 0.0:
            sc = sc + bias
        old = top[i]
        new = jnp.maximum(old, jnp.max(sc, axis=0, keepdims=True))
        p = jnp.exp2(sc - new)
        f = jnp.exp2(old - new)
        top[i] = new
        tot[i] = tot[i] * f + jnp.sum(p, axis=0, keepdims=True)
        acc[i] = acc[i] * f + jnp.dot(values_t, p.astype(BF16), preferred_element_type=F32)

    def block(src):
        def head(i, carry):
            h = i // group
            update(i, kb[src, h], vb[src, h], 0.0)
            return carry

        lax.fori_loop(0, heads, head, 0)

    def wait_from(src):
        for one in copies(src, 0, s):
            one.wait_recv()

    def step(k, carry):
        zz = source(k)
        src = zz * x_count + x

        @pl.when(k > 0)
        def _():
            wait_from(src)

        for way, (ok, peer) in enumerate(targets):
            mine = zz <= z if way == 0 else zz >= z

            @pl.when(ok & mine)
            def _():
                for one in copies(src, way, peer):
                    one.start()

        for j in range(1, x_count):
            for one in copies(src, 1 + j, z * x_count + (x + j) % x_count):
                one.start()
        block(src)

        @pl.when(k > 0)
        def _():
            before = source(k - 1)
            for j in range(1, x_count):
                old = before * x_count + (x + j) % x_count
                wait_from(old)
                block(old)

        return carry

    lax.fori_loop(0, z_count, step, 0)
    final = source(z_count - 1)
    ends = [final * x_count + (x + j) % x_count for j in range(1, x_count)]
    for src in ends:
        copies(src, 0, s)[0].wait_recv()
    for i in range(heads):
        h = i // group
        keys = jnp.concatenate([cb[j, h, 0] for j in range(sp_count)], axis=0)
        vals = jnp.concatenate([cb[j, h, 1] for j in range(sp_count)], axis=0)
        update(i, keys, vals.astype(F32).T.astype(BF16), lift * math.log2(math.e))
    for src in ends:
        for one in copies(src, 0, s)[1:]:
            one.wait_recv()
        block(src)
    for i in range(heads):
        out_ref[:, i * head_dim : (i + 1) * head_dim] = (acc[i] / tot[i]).T.astype(BF16)

    def drain(k, carry):
        zz = source(k)
        src = zz * x_count + x
        for way, (ok, peer) in enumerate(targets):
            mine = zz <= z if way == 0 else zz >= z

            @pl.when(ok & mine)
            def _():
                for one in copies(src, way, peer):
                    one.wait_send()

        for j in range(1, x_count):
            for one in copies(src, 1 + j, z * x_count + (x + j) % x_count):
                one.wait_send()
        return carry

    lax.fori_loop(0, z_count, drain, 0)


def pair_kernel(
    sp_count, x_count, group, lift,
    k_hbm, vt_hbm, ckv_hbm, qt_ref,
    out_ref,
    kb, vb, cb, top, tot, acc, load_sem, qb, ab, send_sem, recv_sem, swap_sem,
):
    s, t = lax.axis_index("sp"), lax.axis_index("tp")
    z, x = s // x_count, s % x_count
    z_count = sp_count // x_count
    heads, head_dim, rows = qt_ref.shape
    factor = head_dim ** (-0.5) * math.log2(math.e)
    mine = z % 2
    mate = (z + 1 - 2 * mine) * x_count + x

    bufs = (cb, kb, vb)
    loads = [
        pltpu.make_async_copy(a, b.at[s], load_sem.at[i])
        for i, (a, b) in enumerate(zip((ckv_hbm, k_hbm, vt_hbm), bufs))
    ]
    for one in loads:
        one.start()
    barrier = pltpu.get_barrier_semaphore()
    targets = []
    for sign in (1, -1):
        ok = (z + sign >= 0) & (z + sign < z_count)
        peer = ((z + sign + z_count) % z_count) * x_count + x
        targets.append((ok, peer))

        @pl.when(ok)
        def _():
            pl.semaphore_signal(barrier, inc=1, device_id=(peer, t), device_id_type=MESH)

    for j in range(1, x_count):
        peer = z * x_count + (x + j) % x_count
        pl.semaphore_signal(barrier, inc=1, device_id=(peer, t), device_id_type=MESH)
    ends_here = (z == 0).astype(jnp.int32) + (z == z_count - 1).astype(jnp.int32)
    pl.semaphore_wait(barrier, x_count + 1 - ends_here)

    swap_q = remote(
        qt_ref.at[pl.ds((1 - mine) * group, group)], qb.at[0],
        swap_sem.at[0], swap_sem.at[1], (mate, t),
    )
    swap_q.start()
    qb[1] = qt_ref[pl.ds(mine * group, group)]
    top[...] = jnp.full_like(top, -1e30)
    tot[...] = jnp.zeros_like(tot)
    acc[...] = jnp.zeros_like(acc)
    for one in loads:
        one.wait()

    def copy(i, src, h, way, peer):
        b = bufs[i]
        return remote(
            b.at[src, h], b.at[src, h], send_sem.at[i, src, h, way], recv_sem.at[i, src, h],
            (peer, t),
        )

    def source(k):
        low = jnp.minimum(z, z_count - 1 - z)
        both = k <= 2 * low
        dist = jnp.where(both, (k + 1) // 2, k - low)
        up = jnp.where(both, k % 2 == 1, z < z_count - 1 - z)
        return jnp.where(up, z + dist, z - dist)

    def reach(h, way, at):
        return at <= z_count - 2 + h if way == 0 else at >= h

    def flow(k, act_recv, act_send):
        zz = source(k)
        src = zz * x_count + x
        for n in range(2):
            for way, (ok, peer) in enumerate(targets):
                side = zz <= z if way == 0 else zz >= z
                h = 1 - n if way == 0 else n
                came = (zz != z) & side & reach(h, way, z)
                goes = ok & side & reach(h, way, z + 1 if way == 0 else z - 1)
                for i in range(3):
                    if act_recv:

                        @pl.when(came)
                        def _():
                            copy(i, src, h, 0, s).wait_recv()

                    @pl.when(goes)
                    def _():
                        act_send(copy(i, src, h, way, peer))

                    @pl.when(side & (h == mine) & ((zz != z) | (way == 0)))
                    def _():
                        for j in range(1, x_count):
                            act_send(
                                copy(i, src, h, 1 + j, z * x_count + (x + j) % x_count)
                            )

    def update(i, queries, keys, values_t, bias):
        sc = jnp.dot(keys, queries, preferred_element_type=F32) * factor
        if bias != 0.0:
            sc = sc + bias
        old = top[i]
        new = jnp.maximum(old, jnp.max(sc, axis=0, keepdims=True))
        p = jnp.exp2(sc - new)
        f = jnp.exp2(old - new)
        top[i] = new
        tot[i] = tot[i] * f + jnp.sum(p, axis=0, keepdims=True)
        acc[i] = acc[i] * f + jnp.dot(values_t, p.astype(BF16), preferred_element_type=F32)

    def block(src):
        def tile(i, carry):
            update(i, qb[i // group, i % group], kb[src, mine], vb[src, mine], 0.0)
            return carry

        lax.fori_loop(0, 2 * group, tile, 0)

    def step(k, carry):
        flow(k, True, lambda one: one.start())

        @pl.when(k == 0)
        def _():
            swap_q.wait_recv()

        block(source(k) * x_count + x)

        @pl.when(k > 0)
        def _():
            before = source(k - 1)
            for j in range(1, x_count):
                old = before * x_count + (x + j) % x_count
                for i in range(3):
                    copy(i, old, mine, 0, s).wait_recv()
                block(old)

        return carry

    lax.fori_loop(0, z_count, step, 0)
    final = source(z_count - 1)
    ends = [final * x_count + (x + j) % x_count for j in range(1, x_count)]
    for src in ends:
        copy(0, src, mine, 0, s).wait_recv()
    keys = jnp.concatenate([cb[j, mine, 0] for j in range(sp_count)], axis=0)
    vals = jnp.concatenate([cb[j, mine, 1] for j in range(sp_count)], axis=0)
    vals = vals.astype(F32).T.astype(BF16)
    for i in range(2 * group):
        update(i, qb[i // group, i % group], keys, vals, lift * math.log2(math.e))
    for src in ends:
        for i in (1, 2):
            copy(i, src, mine, 0, s).wait_recv()
        block(src)
    span = group * head_dim
    for g in range(group):
        ab[0, :, g * head_dim : (g + 1) * head_dim] = (acc[g] / tot[g]).T.astype(BF16)
    swap_a = remote(ab.at[0], ab.at[1], swap_sem.at[2], swap_sem.at[3], (mate, t))
    swap_a.start()
    for g in range(group):
        at = pl.ds(pl.multiple_of(mine * span + g * head_dim, head_dim), head_dim)
        out_ref[:, at] = (acc[group + g] / tot[group + g]).T.astype(BF16)

    def drain(k, carry):
        flow(k, False, lambda one: one.wait_send())
        return carry

    lax.fori_loop(0, z_count, drain, 0)
    swap_a.wait_recv()
    out_ref[:, pl.ds(pl.multiple_of((1 - mine) * span, head_dim), span)] = ab[1]
    swap_q.wait_send()
    swap_a.wait_send()


def mix_kernel(
    tp_count, chunks,
    att_ref, wo_ref, lat_ref, gate_ref,
    out_ref,
    core_out, core_in, mesh_out, mesh_in, mixed, core_send, core_recv, mesh_send, mesh_recv,
):
    s, t = lax.axis_index("sp"), lax.axis_index("tp")
    y, c = t // 2, t % 2
    y_count = tp_count // 2
    partner = y * 2 + 1 - c
    rows, width = lat_ref.shape
    step = width // chunks
    barrier = pltpu.get_barrier_semaphore()
    peers = [((y + j) % y_count) * 2 + c for j in range(1, y_count)]
    for peer in peers + [partner]:
        pl.semaphore_signal(barrier, inc=1, device_id=(s, peer), device_id_type=MESH)
    pl.semaphore_wait(barrier, y_count)

    def piece(n, j, cc):
        yy = (y + j) % y_count
        at = pl.ds(pl.multiple_of((yy * 2 + cc) * rows, rows), rows)
        return jnp.dot(
            att_ref[at, :], wo_ref[:, n * step : (n + 1) * step], preferred_element_type=F32
        )

    order = list(range(1, y_count)) + [0]
    cores = [
        remote(core_out.at[n], core_in.at[n], core_send.at[n], core_recv.at[n], (s, partner))
        for n in range(chunks)
    ]
    sent = []
    for n in range(chunks):
        for j in order:
            core_out[n, j] = piece(n, j, 1 - c).astype(BF16)
        cores[n].start()
    for n in range(chunks):
        mine = [piece(n, j, c) for j in order]
        cores[n].wait_recv()
        for j, value in zip(order, mine):
            value = value + core_in[n, j].astype(F32)
            if j == 0:
                mixed[n] = value
            else:
                mesh_out[n, j - 1] = value.astype(BF16)
                one = remote(
                    mesh_out.at[n, j - 1], mesh_in.at[n, j - 1], mesh_send.at[n, j - 1],
                    mesh_recv.at[n, j - 1], (s, peers[j - 1]),
                )
                one.start()
                sent.append(one)
    for one in sent:
        one.wait_recv()
    square = jnp.zeros((rows, 1), F32)
    for n in range(chunks):
        value = mixed[n]
        for j in range(1, y_count):
            value = value + mesh_in[n, j - 1].astype(F32)
        mixed[n] = value
        square = square + jnp.sum(value * value, axis=-1, keepdims=True)
    inv = lax.rsqrt(square / width + NORM_EPS)
    for n in range(chunks):
        at = slice(n * step, (n + 1) * step)
        out_ref[:, at] = (
            lat_ref[:, at].astype(F32) + gate_ref[:, at] * (mixed[n] * inv)
        ).astype(BF16)
    for one in sent + cores:
        one.wait_send()


ANY = pl.BlockSpec(memory_space=pl.ANY)
VM = pl.BlockSpec(memory_space=pltpu.VMEM)
DMA = pltpu.SemaphoreType.DMA


def body(
    latents,
    context,
    cond,
    ctx_cond,
    mod_weight,
    query_weight,
    key_matrix,
    value_matrix,
    out_weight,
    query_gain,
    key_gain,
):
    sp_count, tp_count = lax.axis_size("sp"), lax.axis_size("tp")
    x_count = row_size(sp_count)
    rows, width = latents.shape
    ctx_rows = context.shape[0]
    head_dim = query_gain.shape[0]
    heads = query_weight.shape[1] // head_dim
    kv_heads = key_matrix.shape[1] // head_dim
    all_rows = rows * tp_count
    mod_cols = mod_weight.shape[1]
    positions = lax.axis_index("sp") * all_rows + jnp.arange(all_rows, dtype=jnp.int32)
    cos, sin = tables(positions, head_dim)
    pair = jnp.concatenate(
        [cond[None], ctx_cond[None], jnp.zeros((6, cond.shape[0]), F32)], axis=0
    )
    sds = jax.ShapeDtypeStruct
    qt, k, vt, ckv, gate = pl.pallas_call(
        functools.partial(front_kernel, sp_count, tp_count, head_dim),
        out_shape=[
            sds((heads, head_dim, all_rows), BF16),
            sds((kv_heads, all_rows, head_dim), BF16),
            sds((kv_heads, head_dim, all_rows), BF16),
            sds((kv_heads, 2, ctx_rows, head_dim), BF16),
            sds((1, width), F32),
        ],
        in_specs=[VM, ANY, ANY, VM, ANY, ANY, ANY, VM, VM, VM, VM],
        out_specs=[VM] * 5,
        scratch_shapes=[
            pltpu.VMEM(mod_weight.shape, F32),
            pltpu.VMEM((tp_count, rows, width), BF16),
            pltpu.VMEM(query_weight.shape, BF16),
            pltpu.VMEM(key_matrix.shape, BF16),
            pltpu.VMEM(value_matrix.shape, BF16),
            pltpu.VMEM((sp_count, 2, mod_cols), F32),
            pltpu.VMEM((tp_count, 2, mod_cols), F32),
            pltpu.VMEM((2, mod_cols * tp_count), F32),
            pltpu.VMEM((2 * rows, width), BF16),
            DMA((5,)),
            DMA((tp_count,)),
            DMA((tp_count,)),
            DMA((sp_count,)),
            DMA((sp_count,)),
            DMA((tp_count,)),
            DMA((tp_count,)),
        ],
        compiler_params=pltpu.CompilerParams(
            collective_id=0, has_side_effects=True, vmem_limit_bytes=VMEM_BYTES
        ),
        name="front",
    )(
        pair, mod_weight, latents, context, query_weight, key_matrix, value_matrix,
        query_gain[None], key_gain[None], cos, sin,
    )

    lift = math.log(sp_count * all_rows / (2.0 * sp_count * ctx_rows))
    group = heads // kv_heads
    paired = kv_heads == 2 and (sp_count // x_count) % 2 == 0
    scratch = [
        pltpu.VMEM((sp_count, kv_heads, all_rows, head_dim), BF16),
        pltpu.VMEM((sp_count, kv_heads, head_dim, all_rows), BF16),
        pltpu.VMEM((sp_count, kv_heads, 2, ctx_rows, head_dim), BF16),
        pltpu.VMEM((heads, 1, all_rows), F32),
        pltpu.VMEM((heads, 1, all_rows), F32),
        pltpu.VMEM((heads, head_dim, all_rows), F32),
        DMA((3,)),
    ]
    if paired:
        scratch += [
            pltpu.VMEM((2, group, head_dim, all_rows), BF16),
            pltpu.VMEM((2, all_rows, group * head_dim), BF16),
            DMA((3, sp_count, 2, x_count + 1)),
            DMA((3, sp_count, 2)),
            DMA((4,)),
        ]
    else:
        scratch += [DMA((3, sp_count, x_count + 1)), DMA((3, sp_count))]
    att = pl.pallas_call(
        functools.partial(
            pair_kernel if paired else attend_kernel, sp_count, x_count, group, lift
        ),
        out_shape=sds((all_rows, heads * head_dim), BF16),
        in_specs=[ANY, ANY, ANY, VM],
        out_specs=VM,
        scratch_shapes=scratch,
        compiler_params=pltpu.CompilerParams(
            collective_id=1, has_side_effects=True, vmem_limit_bytes=VMEM_BYTES
        ),
        name="attend",
    )(k, vt, ckv, qt)

    chunks = 4
    y_count = tp_count // 2
    step = width // chunks
    far = max(y_count - 1, 1)
    return pl.pallas_call(
        functools.partial(mix_kernel, tp_count, chunks),
        out_shape=sds((rows, width), BF16),
        in_specs=[VM] * 4,
        out_specs=VM,
        scratch_shapes=[
            pltpu.VMEM((chunks, y_count, rows, step), BF16),
            pltpu.VMEM((chunks, y_count, rows, step), BF16),
            pltpu.VMEM((chunks, far, rows, step), BF16),
            pltpu.VMEM((chunks, far, rows, step), BF16),
            pltpu.VMEM((chunks, rows, step), F32),
            DMA((chunks,)),
            DMA((chunks,)),
            DMA((chunks, far)),
            DMA((chunks, far)),
        ],
        compiler_params=pltpu.CompilerParams(
            collective_id=2, has_side_effects=True, vmem_limit_bytes=VMEM_BYTES
        ),
        name="mix",
    )(att, out_weight, latents, gate)


def solution(mesh):
    placed = (
        P(("sp", "tp"), None),
        P("sp", None),
        P("sp"),
        P("sp"),
        P("sp", "tp"),
        P(None, "tp"),
        P(None, "tp"),
        P(None, "tp"),
        P("tp", None),
        P(),
        P(),
    )
    return jax.shard_map(
        body, mesh=mesh, in_specs=placed, out_specs=P(("sp", "tp"), None), check_vma=False
    )
```

```python
import functools
import math

import jax
import jax.numpy as jnp
from jax import lax
from jax.experimental import pallas as pl
from jax.experimental.pallas import tpu as pltpu
from jax.sharding import PartitionSpec as P

GRID_W = 64
NORM_EPS = 1e-06
ROPE_BASE = 10000.0
MESH = pl.DeviceIdType.MESH
BF16 = jnp.bfloat16
F32 = jnp.float32
VMEM_BYTES = 67043328


def row_size(sp_count):
    size = 1
    while 4 * size * size <= sp_count:
        size *= 2
    return size


def tables(positions, head_dim):
    quarter = head_dim // 4
    inv_freq = ROPE_BASE ** (-jnp.arange(quarter, dtype=F32) / quarter)
    where = jnp.stack([positions // GRID_W, positions % GRID_W]).astype(F32)
    angles = where[:, None, :] * inv_freq[None, :, None]
    return jnp.cos(angles), jnp.sin(angles)


def remote(src, dst, send, recv, dev):
    return pltpu.make_async_remote_copy(
        src_ref=src, dst_ref=dst, send_sem=send, recv_sem=recv, device_id=dev, device_id_type=MESH
    )


def front_kernel(
    sp_count, tp_count, head_dim,
    cond_ref, mw_hbm, lat_hbm, ctx_ref, wq_hbm, wk_hbm, wv_hbm, qg_ref, kg_ref, cos_ref, sin_ref,
    qt_ref, k_ref, vt_ref, ckv_ref, gate_ref,
    mw, lat, wq, wk, wv, part, tot, mod, xn, load_sem,
    lat_send, lat_recv, part_send, part_recv, tot_send, tot_recv,
):
    s, t = lax.axis_index("sp"), lax.axis_index("tp")
    y, c = t // 2, t % 2
    y_count = tp_count // 2
    partner = y * 2 + 1 - c
    rows = lat.shape[1]
    width = lat.shape[2]
    model_cols = mod.shape[1]

    own = pltpu.make_async_copy(lat_hbm, lat.at[t], load_sem.at[0])
    own.start()
    loads = [
        pltpu.make_async_copy(a, b, load_sem.at[1 + i])
        for i, (a, b) in enumerate(((mw_hbm, mw), (wq_hbm, wq), (wk_hbm, wk), (wv_hbm, wv)))
    ]
    for one in loads:
        one.start()

    barrier = pltpu.get_barrier_semaphore()
    for j in range(1, sp_count):
        pl.semaphore_signal(barrier, inc=1, device_id=((s + j) % sp_count, t), device_id_type=MESH)
    for j in range(1, tp_count):
        pl.semaphore_signal(barrier, inc=1, device_id=(s, (t + j) % tp_count), device_id_type=MESH)
    pl.semaphore_wait(barrier, sp_count + tp_count - 2)

    own.wait()
    sends = []
    for j in range(1, y_count):
        peer = ((y + j) % y_count) * 2 + c
        sends.append(remote(lat.at[t], lat.at[t], lat_send.at[j], lat_recv.at[t], (s, peer)))
    sends.append(remote(lat.at[t], lat.at[t], lat_send.at[0], lat_recv.at[t], (s, partner)))
    for one in sends:
        one.start()

    loads[0].wait()
    cond = cond_ref[...]
    cond = cond * jax.nn.sigmoid(cond)
    part[s] = jnp.dot(
        cond, mw[...], precision=lax.Precision.HIGHEST, preferred_element_type=F32
    )[:2]
    more = [
        remote(part.at[s], part.at[s], part_send.at[j], part_recv.at[s], ((s + j) % sp_count, t))
        for j in range(1, sp_count)
    ]
    for one in more:
        one.start()
    for j in range(1, sp_count):
        src = (s + j) % sp_count
        remote(part.at[src], part.at[src], part_send.at[0], part_recv.at[src], (s, t)).wait_recv()
    total = part[0]
    for j in range(1, sp_count):
        total = total + part[j]
    tot[t] = total
    last = [
        remote(tot.at[t], tot.at[t], tot_send.at[j], tot_recv.at[t], (s, (t + j) % tp_count))
        for j in range(1, tp_count)
    ]
    for one in last:
        one.start()
    for j in range(1, tp_count):
        src = (t + j) % tp_count
        remote(tot.at[src], tot.at[src], tot_send.at[0], tot_recv.at[src], (s, t)).wait_recv()
    cols = model_cols // tp_count
    for j in range(tp_count):
        mod[:, j * cols : (j + 1) * cols] = tot[j]
    gate_ref[...] = mod[0:1, 2 * width :]

    def modulate(x, r):
        x = x.astype(F32)
        scaled = x * lax.rsqrt(jnp.mean(x * x, axis=-1, keepdims=True) + NORM_EPS)
        shift, scale = mod[r : r + 1, :width], mod[r : r + 1, width : 2 * width]
        return (scaled * (1.0 + scale) + shift).astype(BF16)

    for one in loads[1:]:
        one.wait()

    cn = modulate(ctx_ref[...], 1)
    kc = jnp.dot(cn, wk[...], preferred_element_type=F32)
    vc = jnp.dot(cn, wv[...], preferred_element_type=F32)
    for h in range(kc.shape[1] // head_dim):
        kh = kc[:, h * head_dim : (h + 1) * head_dim]
        kh = kh * lax.rsqrt(jnp.mean(kh * kh, axis=-1, keepdims=True) + NORM_EPS) * kg_ref[...]
        ckv_ref[h, 0] = kh.astype(BF16)
        ckv_ref[h, 1] = vc[:, h * head_dim : (h + 1) * head_dim].astype(BF16)

    q4 = head_dim // 4
    qgain, kgain = qg_ref[...], kg_ref[...]

    def turn(yt, cos, sin):
        out = []
        for n in range(2):
            a = yt[2 * n * q4 : (2 * n + 1) * q4]
            b = yt[(2 * n + 1) * q4 : (2 * n + 2) * q4]
            out += [a * cos[n] - b * sin[n], b * cos[n] + a * sin[n]]
        return jnp.concatenate(out, axis=0)

    def unit(yh, gain):
        return yh * lax.rsqrt(jnp.mean(yh * yh, axis=-1, keepdims=True) + NORM_EPS) * gain

    span = 2 * rows
    relays = []
    for j in range(y_count):
        yy = (y + j) % y_count
        if j > 0:
            src = yy * 2 + c
            remote(lat.at[src], lat.at[src], lat_send.at[0], lat_recv.at[src], (s, t)).wait_recv()
            one = remote(
                lat.at[src], lat.at[src], lat_send.at[y_count - 1 + j], lat_recv.at[src], (s, partner)
            )
            one.start()
            relays.append(one)
        other = yy * 2 + 1 - c
        remote(lat.at[other], lat.at[other], lat_send.at[0], lat_recv.at[other], (s, t)).wait_recv()
        for i in range(2):
            xn[i * rows : (i + 1) * rows, :] = modulate(lat[yy * 2 + i], 0)
        x = xn[...]
        at = pl.ds(pl.multiple_of(yy * span, span), span)
        cos, sin = cos_ref[:, :, at], sin_ref[:, :, at]
        for w, kind in ((wq, 0), (wk, 1), (wv, 2)):
            step = min(2 * head_dim, w.shape[1])
            for n in range(0, w.shape[1], step):
                full = jnp.dot(x, w[:, n : n + step], preferred_element_type=F32)
                for m in range(0, step, head_dim):
                    h = (n + m) // head_dim
                    yh = full[:, m : m + head_dim]
                    if kind == 0:
                        qt_ref[h, :, at] = turn(unit(yh, qgain).T, cos, sin).astype(BF16)
                    elif kind == 1:
                        k_ref[h, at, :] = turn(unit(yh, kgain).T, cos, sin).T.astype(BF16)
                    else:
                        vt_ref[h, :, at] = yh.T.astype(BF16)
    for one in sends + more + last + relays:
        one.wait_send()


def attend_kernel(
    sp_count, x_count, group, lift,
    k_hbm, vt_hbm, ckv_hbm, qt_ref,
    out_ref,
    kb, vb, cb, top, tot, acc, load_sem, send_sem, recv_sem,
):
    s, t = lax.axis_index("sp"), lax.axis_index("tp")
    z, x = s // x_count, s % x_count
    z_count = sp_count // x_count
    heads, head_dim, rows = qt_ref.shape
    kv_heads = heads // group
    factor = head_dim ** (-0.5) * math.log2(math.e)

    loads = [
        pltpu.make_async_copy(a, b, load_sem.at[i])
        for i, (a, b) in enumerate(
            (
                (ckv_hbm, cb.at[s]),
                (k_hbm, kb.at[s]),
                (vt_hbm, vb.at[s]),
            )
        )
    ]
    for one in loads:
        one.start()
    barrier = pltpu.get_barrier_semaphore()
    targets = []
    for sign in (1, -1):
        ok = (z + sign >= 0) & (z + sign < z_count)
        peer = ((z + sign + z_count) % z_count) * x_count + x
        targets.append((ok, peer))
    for ok, peer in targets:

        @pl.when(ok)
        def _():
            pl.semaphore_signal(barrier, inc=1, device_id=(peer, t), device_id_type=MESH)

    for j in range(1, x_count):
        peer = z * x_count + (x + j) % x_count
        pl.semaphore_signal(barrier, inc=1, device_id=(peer, t), device_id_type=MESH)
    ends_here = (z == 0).astype(jnp.int32) + (z == z_count - 1).astype(jnp.int32)
    pl.semaphore_wait(barrier, x_count + 1 - ends_here)

    top[...] = jnp.full_like(top, -1e30)
    tot[...] = jnp.zeros_like(tot)
    acc[...] = jnp.zeros_like(acc)
    for one in loads:
        one.wait()

    bufs = (cb, kb, vb)

    def copies(src, way, peer):
        return [
            remote(b.at[src], b.at[src], send_sem.at[i, src, way], recv_sem.at[i, src], (peer, t))
            for i, b in enumerate(bufs)
        ]

    def source(k):
        low = jnp.minimum(z, z_count - 1 - z)
        both = k <= 2 * low
        dist = jnp.where(both, (k + 1) // 2, k - low)
        up = jnp.where(both, k % 2 == 1, z < z_count - 1 - z)
        return jnp.where(up, z + dist, z - dist)

    def update(i, keys, values_t, bias):
        sc = jnp.dot(keys, qt_ref[i], preferred_element_type=F32) * factor
        if bias != 0.0:
            sc = sc + bias
        old = top[i]
        new = jnp.maximum(old, jnp.max(sc, axis=0, keepdims=True))
        p = jnp.exp2(sc - new)
        f = jnp.exp2(old - new)
        top[i] = new
        tot[i] = tot[i] * f + jnp.sum(p, axis=0, keepdims=True)
        acc[i] = acc[i] * f + jnp.dot(values_t, p.astype(BF16), preferred_element_type=F32)

    def block(src):
        def head(i, carry):
            h = i // group
            update(i, kb[src, h], vb[src, h], 0.0)
            return carry

        lax.fori_loop(0, heads, head, 0)

    def wait_from(src):
        for one in copies(src, 0, s):
            one.wait_recv()

    def step(k, carry):
        zz = source(k)
        src = zz * x_count + x

        @pl.when(k > 0)
        def _():
            wait_from(src)

        for way, (ok, peer) in enumerate(targets):
            mine = zz <= z if way == 0 else zz >= z

            @pl.when(ok & mine)
            def _():
                for one in copies(src, way, peer):
                    one.start()

        for j in range(1, x_count):
            for one in copies(src, 1 + j, z * x_count + (x + j) % x_count):
                one.start()
        block(src)

        @pl.when(k > 0)
        def _():
            before = source(k - 1)
            for j in range(1, x_count):
                old = before * x_count + (x + j) % x_count
                wait_from(old)
                block(old)

        return carry

    lax.fori_loop(0, z_count, step, 0)
    final = source(z_count - 1)
    ends = [final * x_count + (x + j) % x_count for j in range(1, x_count)]
    for src in ends:
        copies(src, 0, s)[0].wait_recv()
    for i in range(heads):
        h = i // group
        keys = jnp.concatenate([cb[j, h, 0] for j in range(sp_count)], axis=0)
        vals = jnp.concatenate([cb[j, h, 1] for j in range(sp_count)], axis=0)
        update(i, keys, vals.astype(F32).T.astype(BF16), lift * math.log2(math.e))
    for src in ends:
        for one in copies(src, 0, s)[1:]:
            one.wait_recv()
        block(src)
    for i in range(heads):
        out_ref[:, i * head_dim : (i + 1) * head_dim] = (acc[i] / tot[i]).T.astype(BF16)

    def drain(k, carry):
        zz = source(k)
        src = zz * x_count + x
        for way, (ok, peer) in enumerate(targets):
            mine = zz <= z if way == 0 else zz >= z

            @pl.when(ok & mine)
            def _():
                for one in copies(src, way, peer):
                    one.wait_send()

        for j in range(1, x_count):
            for one in copies(src, 1 + j, z * x_count + (x + j) % x_count):
                one.wait_send()
        return carry

    lax.fori_loop(0, z_count, drain, 0)


def pair_kernel(
    sp_count, x_count, group, lift,
    k_hbm, vt_hbm, ckv_hbm, qt_ref,
    out_ref,
    kb, vb, cb, top, tot, acc, load_sem, qb, ab, send_sem, recv_sem, swap_sem,
):
    s, t = lax.axis_index("sp"), lax.axis_index("tp")
    z, x = s // x_count, s % x_count
    z_count = sp_count // x_count
    heads, head_dim, rows = qt_ref.shape
    factor = head_dim ** (-0.5) * math.log2(math.e)
    mine = z % 2
    mate = (z + 1 - 2 * mine) * x_count + x

    bufs = (cb, kb, vb)
    loads = [
        pltpu.make_async_copy(a, b.at[s], load_sem.at[i])
        for i, (a, b) in enumerate(zip((ckv_hbm, k_hbm, vt_hbm), bufs))
    ]
    for one in loads:
        one.start()
    barrier = pltpu.get_barrier_semaphore()
    for j in range(1, z_count):
        peer = (z + j) % z_count * x_count + x
        pl.semaphore_signal(barrier, inc=1, device_id=(peer, t), device_id_type=MESH)
    for j in range(1, x_count):
        peer = z * x_count + (x + j) % x_count
        pl.semaphore_signal(barrier, inc=1, device_id=(peer, t), device_id_type=MESH)
    pl.semaphore_wait(barrier, x_count + z_count - 2)

    swap_q = remote(
        qt_ref.at[pl.ds((1 - mine) * group, group)], qb.at[0],
        swap_sem.at[0], swap_sem.at[1], (mate, t),
    )
    swap_q.start()
    qb[1] = qt_ref[pl.ds(mine * group, group)]
    top[...] = jnp.full_like(top, -1e30)
    tot[...] = jnp.zeros_like(tot)
    acc[...] = jnp.zeros_like(acc)
    for one in loads:
        one.wait()

    def copy(i, src, h, way, peer):
        b = bufs[i]
        return remote(
            b.at[src, h], b.at[src, h], send_sem.at[i, way], recv_sem.at[i, src], (peer, t)
        )

    def source(k):
        low = jnp.minimum(z, z_count - 1 - z)
        both = k <= 2 * low
        dist = jnp.where(both, (k + 1) // 2, k - low)
        up = jnp.where(both, k % 2 == 1, z < z_count - 1 - z)
        return jnp.where(up, z + dist, z - dist)

    def line(act):
        for dist in range(1, z_count):
            for sign in (1, -1):
                there = z + sign * dist

                @pl.when((there >= 0) & (there < z_count))
                def _():
                    to = (there + z_count) % z_count
                    for i in range(3):
                        act(copy(i, s, to % 2, to, to * x_count + x))

    def across(k, act):
        zz = source(k)
        src = zz * x_count + x
        for i in range(3):
            if act is None:

                @pl.when(k > 0)
                def _():
                    copy(i, src, mine, 0, s).wait_recv()

            for j in range(1, x_count):
                way = z_count + zz * (x_count - 1) + j - 1
                one = copy(i, src, mine, way, z * x_count + (x + j) % x_count)
                one.start() if act is None else act(one)

    def update(i, queries, keys, values_t, bias):
        sc = jnp.dot(keys, queries, preferred_element_type=F32) * factor
        if bias != 0.0:
            sc = sc + bias
        old = top[i]
        new = jnp.maximum(old, jnp.max(sc, axis=0, keepdims=True))
        p = jnp.exp2(sc - new)
        f = jnp.exp2(old - new)
        top[i] = new
        tot[i] = tot[i] * f + jnp.sum(p, axis=0, keepdims=True)
        acc[i] = acc[i] * f + jnp.dot(values_t, p.astype(BF16), preferred_element_type=F32)

    def block(src):
        def tile(i, carry):
            update(i, qb[i // group, i % group], kb[src, mine], vb[src, mine], 0.0)
            return carry

        lax.fori_loop(0, 2 * group, tile, 0)

    def step(k, carry):
        across(k, None)

        @pl.when(k == 0)
        def _():
            swap_q.wait_recv()

        block(source(k) * x_count + x)

        @pl.when(k > 0)
        def _():
            before = source(k - 1)
            for j in range(1, x_count):
                old = before * x_count + (x + j) % x_count
                for i in range(3):
                    copy(i, old, mine, 0, s).wait_recv()
                block(old)

        return carry

    line(lambda one: one.start())
    lax.fori_loop(0, z_count, step, 0)
    final = source(z_count - 1)
    ends = [final * x_count + (x + j) % x_count for j in range(1, x_count)]
    for src in ends:
        copy(0, src, mine, 0, s).wait_recv()
    keys = jnp.concatenate([cb[j, mine, 0] for j in range(sp_count)], axis=0)
    vals = jnp.concatenate([cb[j, mine, 1] for j in range(sp_count)], axis=0)
    vals = vals.astype(F32).T.astype(BF16)
    span = group * head_dim
    swap_a = remote(ab.at[0], ab.at[1], swap_sem.at[2], swap_sem.at[3], (mate, t))
    for who in range(2):
        for g in range(group):
            update(who * group + g, qb[who, g], keys, vals, lift * math.log2(math.e))
        for src in ends:
            if who == 0:
                for i in (1, 2):
                    copy(i, src, mine, 0, s).wait_recv()
            for g in range(group):
                update(who * group + g, qb[who, g], kb[src, mine], vb[src, mine], 0.0)
        for g in range(group):
            i = who * group + g
            done = (acc[i] / tot[i]).T.astype(BF16)
            if who == 0:
                ab[0, :, g * head_dim : (g + 1) * head_dim] = done
            else:
                at = pl.ds(pl.multiple_of(mine * span + g * head_dim, head_dim), head_dim)
                out_ref[:, at] = done
        if who == 0:
            swap_a.start()

    def drain(k, carry):
        across(k, lambda one: one.wait_send())
        return carry

    lax.fori_loop(0, z_count, drain, 0)
    line(lambda one: one.wait_send())
    swap_a.wait_recv()
    out_ref[:, pl.ds(pl.multiple_of((1 - mine) * span, head_dim), span)] = ab[1]
    swap_q.wait_send()
    swap_a.wait_send()


def mix_kernel(
    tp_count, chunks,
    att_ref, wo_ref, lat_ref, gate_ref,
    out_ref,
    core_out, core_in, mesh_out, mesh_in, mixed, core_send, core_recv, mesh_send, mesh_recv,
):
    s, t = lax.axis_index("sp"), lax.axis_index("tp")
    y, c = t // 2, t % 2
    y_count = tp_count // 2
    partner = y * 2 + 1 - c
    rows, width = lat_ref.shape
    step = width // chunks
    barrier = pltpu.get_barrier_semaphore()
    peers = [((y + j) % y_count) * 2 + c for j in range(1, y_count)]
    for peer in peers + [partner]:
        pl.semaphore_signal(barrier, inc=1, device_id=(s, peer), device_id_type=MESH)
    pl.semaphore_wait(barrier, y_count)

    def piece(n, j, cc):
        yy = (y + j) % y_count
        at = pl.ds(pl.multiple_of((yy * 2 + cc) * rows, rows), rows)
        return jnp.dot(
            att_ref[at, :], wo_ref[:, n * step : (n + 1) * step], preferred_element_type=F32
        )

    order = list(range(1, y_count)) + [0]
    cores = [
        remote(core_out.at[n], core_in.at[n], core_send.at[n], core_recv.at[n], (s, partner))
        for n in range(chunks)
    ]
    sent = []
    for n in range(chunks):
        for j in order:
            core_out[n, j] = piece(n, j, 1 - c).astype(BF16)
        cores[n].start()
    for n in range(chunks):
        mine = [piece(n, j, c) for j in order]
        cores[n].wait_recv()
        for j, value in zip(order, mine):
            value = value + core_in[n, j].astype(F32)
            if j == 0:
                mixed[n] = value
            else:
                mesh_out[n, j - 1] = value.astype(BF16)
                one = remote(
                    mesh_out.at[n, j - 1], mesh_in.at[n, j - 1], mesh_send.at[n, j - 1],
                    mesh_recv.at[n, j - 1], (s, peers[j - 1]),
                )
                one.start()
                sent.append(one)
    for one in sent:
        one.wait_recv()
    square = jnp.zeros((rows, 1), F32)
    for n in range(chunks):
        value = mixed[n]
        for j in range(1, y_count):
            value = value + mesh_in[n, j - 1].astype(F32)
        mixed[n] = value
        square = square + jnp.sum(value * value, axis=-1, keepdims=True)
    inv = lax.rsqrt(square / width + NORM_EPS)
    for n in range(chunks):
        at = slice(n * step, (n + 1) * step)
        out_ref[:, at] = (
            lat_ref[:, at].astype(F32) + gate_ref[:, at] * (mixed[n] * inv)
        ).astype(BF16)
    for one in sent + cores:
        one.wait_send()


ANY = pl.BlockSpec(memory_space=pl.ANY)
VM = pl.BlockSpec(memory_space=pltpu.VMEM)
DMA = pltpu.SemaphoreType.DMA


def body(
    latents,
    context,
    cond,
    ctx_cond,
    mod_weight,
    query_weight,
    key_matrix,
    value_matrix,
    out_weight,
    query_gain,
    key_gain,
):
    sp_count, tp_count = lax.axis_size("sp"), lax.axis_size("tp")
    x_count = row_size(sp_count)
    rows, width = latents.shape
    ctx_rows = context.shape[0]
    head_dim = query_gain.shape[0]
    heads = query_weight.shape[1] // head_dim
    kv_heads = key_matrix.shape[1] // head_dim
    all_rows = rows * tp_count
    mod_cols = mod_weight.shape[1]
    positions = lax.axis_index("sp") * all_rows + jnp.arange(all_rows, dtype=jnp.int32)
    cos, sin = tables(positions, head_dim)
    pair = jnp.concatenate(
        [cond[None], ctx_cond[None], jnp.zeros((6, cond.shape[0]), F32)], axis=0
    )
    sds = jax.ShapeDtypeStruct
    qt, k, vt, ckv, gate = pl.pallas_call(
        functools.partial(front_kernel, sp_count, tp_count, head_dim),
        out_shape=[
            sds((heads, head_dim, all_rows), BF16),
            sds((kv_heads, all_rows, head_dim), BF16),
            sds((kv_heads, head_dim, all_rows), BF16),
            sds((kv_heads, 2, ctx_rows, head_dim), BF16),
            sds((1, width), F32),
        ],
        in_specs=[VM, ANY, ANY, VM, ANY, ANY, ANY, VM, VM, VM, VM],
        out_specs=[VM] * 5,
        scratch_shapes=[
            pltpu.VMEM(mod_weight.shape, F32),
            pltpu.VMEM((tp_count, rows, width), BF16),
            pltpu.VMEM(query_weight.shape, BF16),
            pltpu.VMEM(key_matrix.shape, BF16),
            pltpu.VMEM(value_matrix.shape, BF16),
            pltpu.VMEM((sp_count, 2, mod_cols), F32),
            pltpu.VMEM((tp_count, 2, mod_cols), F32),
            pltpu.VMEM((2, mod_cols * tp_count), F32),
            pltpu.VMEM((2 * rows, width), BF16),
            DMA((5,)),
            DMA((tp_count,)),
            DMA((tp_count,)),
            DMA((sp_count,)),
            DMA((sp_count,)),
            DMA((tp_count,)),
            DMA((tp_count,)),
        ],
        compiler_params=pltpu.CompilerParams(
            collective_id=0, has_side_effects=True, vmem_limit_bytes=VMEM_BYTES
        ),
        name="front",
    )(
        pair, mod_weight, latents, context, query_weight, key_matrix, value_matrix,
        query_gain[None], key_gain[None], cos, sin,
    )

    lift = math.log(sp_count * all_rows / (2.0 * sp_count * ctx_rows))
    group = heads // kv_heads
    paired = kv_heads == 2 and (sp_count // x_count) % 2 == 0
    scratch = [
        pltpu.VMEM((sp_count, kv_heads, all_rows, head_dim), BF16),
        pltpu.VMEM((sp_count, kv_heads, head_dim, all_rows), BF16),
        pltpu.VMEM((sp_count, kv_heads, 2, ctx_rows, head_dim), BF16),
        pltpu.VMEM((heads, 1, all_rows), F32),
        pltpu.VMEM((heads, 1, all_rows), F32),
        pltpu.VMEM((heads, head_dim, all_rows), F32),
        DMA((3,)),
    ]
    if paired:
        scratch += [
            pltpu.VMEM((2, group, head_dim, all_rows), BF16),
            pltpu.VMEM((2, all_rows, group * head_dim), BF16),
            DMA((3, sp_count)),
            DMA((3, sp_count)),
            DMA((4,)),
        ]
    else:
        scratch += [DMA((3, sp_count, x_count + 1)), DMA((3, sp_count))]
    att = pl.pallas_call(
        functools.partial(
            pair_kernel if paired else attend_kernel, sp_count, x_count, group, lift
        ),
        out_shape=sds((all_rows, heads * head_dim), BF16),
        in_specs=[ANY, ANY, ANY, VM],
        out_specs=VM,
        scratch_shapes=scratch,
        compiler_params=pltpu.CompilerParams(
            collective_id=1, has_side_effects=True, vmem_limit_bytes=VMEM_BYTES
        ),
        name="attend",
    )(k, vt, ckv, qt)

    chunks = 4
    y_count = tp_count // 2
    step = width // chunks
    far = max(y_count - 1, 1)
    return pl.pallas_call(
        functools.partial(mix_kernel, tp_count, chunks),
        out_shape=sds((rows, width), BF16),
        in_specs=[VM] * 4,
        out_specs=VM,
        scratch_shapes=[
            pltpu.VMEM((chunks, y_count, rows, step), BF16),
            pltpu.VMEM((chunks, y_count, rows, step), BF16),
            pltpu.VMEM((chunks, far, rows, step), BF16),
            pltpu.VMEM((chunks, far, rows, step), BF16),
            pltpu.VMEM((chunks, rows, step), F32),
            DMA((chunks,)),
            DMA((chunks,)),
            DMA((chunks, far)),
            DMA((chunks, far)),
        ],
        compiler_params=pltpu.CompilerParams(
            collective_id=2, has_side_effects=True, vmem_limit_bytes=40 << 20
        ),
        name="mix",
    )(att, out_weight, latents, gate)


def solution(mesh):
    placed = (
        P(("sp", "tp"), None),
        P("sp", None),
        P("sp"),
        P("sp"),
        P("sp", "tp"),
        P(None, "tp"),
        P(None, "tp"),
        P(None, "tp"),
        P("tp", None),
        P(),
        P(),
    )
    return jax.shard_map(
        body, mesh=mesh, in_specs=placed, out_specs=P(("sp", "tp"), None), check_vma=False
    )
```

```python
import functools
import math

import jax
import jax.numpy as jnp
from jax import lax
from jax.experimental import pallas as pl
from jax.experimental.pallas import tpu as pltpu
from jax.sharding import PartitionSpec as P

GRID_W = 64
NORM_EPS = 1e-06
ROPE_BASE = 10000.0
MESH = pl.DeviceIdType.MESH
BF16 = jnp.bfloat16
F32 = jnp.float32
VMEM_BYTES = 67043328


def row_size(sp_count):
    size = 1
    while 4 * size * size <= sp_count:
        size *= 2
    return size


def tables(positions, head_dim):
    quarter = head_dim // 4
    inv_freq = ROPE_BASE ** (-jnp.arange(quarter, dtype=F32) / quarter)
    where = jnp.stack([positions // GRID_W, positions % GRID_W]).astype(F32)
    angles = where[:, None, :] * inv_freq[None, :, None]
    return jnp.cos(angles), jnp.sin(angles)


def remote(src, dst, send, recv, dev):
    return pltpu.make_async_remote_copy(
        src_ref=src, dst_ref=dst, send_sem=send, recv_sem=recv, device_id=dev, device_id_type=MESH
    )


def front_kernel(
    sp_count, tp_count, head_dim,
    cond_ref, mw_hbm, lat_hbm, ctx_ref, wq_hbm, wk_hbm, wv_hbm, qg_ref, kg_ref, cos_ref, sin_ref,
    qt_ref, k_ref, vt_ref, ckv_ref, gate_ref,
    mw, lat, wq, wk, wv, part, tot, mod, xn, load_sem,
    lat_send, lat_recv, part_send, part_recv, tot_send, tot_recv,
    wo_hbm, wo_vm, wo_sem,
):
    s, t = lax.axis_index("sp"), lax.axis_index("tp")
    y, c = t // 2, t % 2
    y_count = tp_count // 2
    partner = y * 2 + 1 - c
    rows = lat.shape[1]
    width = lat.shape[2]
    model_cols = mod.shape[1]

    own = pltpu.make_async_copy(lat_hbm, lat.at[t], load_sem.at[0])
    own.start()
    loads = [
        pltpu.make_async_copy(a, b, load_sem.at[1 + i])
        for i, (a, b) in enumerate(((mw_hbm, mw), (wq_hbm, wq), (wk_hbm, wk), (wv_hbm, wv)))
    ]
    for one in loads:
        one.start()

    pltpu.make_async_copy(wo_hbm, wo_vm, wo_sem.at[0]).start()

    barrier = pltpu.get_barrier_semaphore()
    for j in range(1, sp_count):
        pl.semaphore_signal(barrier, inc=1, device_id=((s + j) % sp_count, t), device_id_type=MESH)
    for j in range(1, tp_count):
        pl.semaphore_signal(barrier, inc=1, device_id=(s, (t + j) % tp_count), device_id_type=MESH)
    pl.semaphore_wait(barrier, sp_count + tp_count - 2)

    own.wait()
    sends = []
    for j in range(1, y_count):
        peer = ((y + j) % y_count) * 2 + c
        sends.append(remote(lat.at[t], lat.at[t], lat_send.at[j], lat_recv.at[t], (s, peer)))
    sends.append(remote(lat.at[t], lat.at[t], lat_send.at[0], lat_recv.at[t], (s, partner)))
    for one in sends:
        one.start()

    loads[0].wait()
    cond = cond_ref[...]
    cond = cond * jax.nn.sigmoid(cond)
    part[s] = jnp.dot(
        cond, mw[...], precision=lax.Precision.HIGHEST, preferred_element_type=F32
    )[:2]
    more = [
        remote(part.at[s], part.at[s], part_send.at[j], part_recv.at[s], ((s + j) % sp_count, t))
        for j in range(1, sp_count)
    ]
    for one in more:
        one.start()
    for j in range(1, sp_count):
        src = (s + j) % sp_count
        remote(part.at[src], part.at[src], part_send.at[0], part_recv.at[src], (s, t)).wait_recv()
    total = part[0]
    for j in range(1, sp_count):
        total = total + part[j]
    tot[t] = total
    last = [
        remote(tot.at[t], tot.at[t], tot_send.at[j], tot_recv.at[t], (s, (t + j) % tp_count))
        for j in range(1, tp_count)
    ]
    for one in last:
        one.start()
    for j in range(1, tp_count):
        src = (t + j) % tp_count
        remote(tot.at[src], tot.at[src], tot_send.at[0], tot_recv.at[src], (s, t)).wait_recv()
    cols = model_cols // tp_count
    for j in range(tp_count):
        mod[:, j * cols : (j + 1) * cols] = tot[j]
    gate_ref[...] = mod[0:1, 2 * width :]

    def modulate(x, r):
        x = x.astype(F32)
        scaled = x * lax.rsqrt(jnp.mean(x * x, axis=-1, keepdims=True) + NORM_EPS)
        shift, scale = mod[r : r + 1, :width], mod[r : r + 1, width : 2 * width]
        return (scaled * (1.0 + scale) + shift).astype(BF16)

    for one in loads[1:]:
        one.wait()

    cn = modulate(ctx_ref[...], 1)
    kc = jnp.dot(cn, wk[...], preferred_element_type=F32)
    vc = jnp.dot(cn, wv[...], preferred_element_type=F32)
    for h in range(kc.shape[1] // head_dim):
        kh = kc[:, h * head_dim : (h + 1) * head_dim]
        kh = kh * lax.rsqrt(jnp.mean(kh * kh, axis=-1, keepdims=True) + NORM_EPS) * kg_ref[...]
        ckv_ref[h, 0] = kh.astype(BF16)
        ckv_ref[h, 1] = vc[:, h * head_dim : (h + 1) * head_dim].astype(BF16)

    q4 = head_dim // 4
    qgain, kgain = qg_ref[...], kg_ref[...]

    def turn(yt, cos, sin):
        out = []
        for n in range(2):
            a = yt[2 * n * q4 : (2 * n + 1) * q4]
            b = yt[(2 * n + 1) * q4 : (2 * n + 2) * q4]
            out += [a * cos[n] - b * sin[n], b * cos[n] + a * sin[n]]
        return jnp.concatenate(out, axis=0)

    def unit(yh, gain):
        return yh * lax.rsqrt(jnp.mean(yh * yh, axis=-1, keepdims=True) + NORM_EPS) * gain

    span = 2 * rows
    relays = []
    for j in range(y_count):
        yy = (y + j) % y_count
        if j > 0:
            src = yy * 2 + c
            remote(lat.at[src], lat.at[src], lat_send.at[0], lat_recv.at[src], (s, t)).wait_recv()
            one = remote(
                lat.at[src], lat.at[src], lat_send.at[y_count - 1 + j], lat_recv.at[src], (s, partner)
            )
            one.start()
            relays.append(one)
        other = yy * 2 + 1 - c
        remote(lat.at[other], lat.at[other], lat_send.at[0], lat_recv.at[other], (s, t)).wait_recv()
        for i in range(2):
            xn[i * rows : (i + 1) * rows, :] = modulate(lat[yy * 2 + i], 0)
        x = xn[...]
        at = pl.ds(pl.multiple_of(yy * span, span), span)
        cos, sin = cos_ref[:, :, at], sin_ref[:, :, at]
        for w, kind in ((wq, 0), (wk, 1), (wv, 2)):
            step = min(2 * head_dim, w.shape[1])
            for n in range(0, w.shape[1], step):
                full = jnp.dot(x, w[:, n : n + step], preferred_element_type=F32)
                for m in range(0, step, head_dim):
                    h = (n + m) // head_dim
                    yh = full[:, m : m + head_dim]
                    if kind == 0:
                        qt_ref[h, :, at] = turn(unit(yh, qgain).T, cos, sin).astype(BF16)
                    elif kind == 1:
                        k_ref[h, at, :] = turn(unit(yh, kgain).T, cos, sin).T.astype(BF16)
                    else:
                        vt_ref[h, :, at] = yh.T.astype(BF16)
    for one in sends + more + last + relays:
        one.wait_send()


def attend_kernel(
    sp_count, x_count, group, lift,
    k_hbm, vt_hbm, ckv_hbm, qt_ref,
    out_ref,
    kb, vb, cb, top, tot, acc, load_sem, send_sem, recv_sem,
):
    s, t = lax.axis_index("sp"), lax.axis_index("tp")
    z, x = s // x_count, s % x_count
    z_count = sp_count // x_count
    heads, head_dim, rows = qt_ref.shape
    kv_heads = heads // group
    factor = head_dim ** (-0.5) * math.log2(math.e)

    loads = [
        pltpu.make_async_copy(a, b, load_sem.at[i])
        for i, (a, b) in enumerate(
            (
                (ckv_hbm, cb.at[s]),
                (k_hbm, kb.at[s]),
                (vt_hbm, vb.at[s]),
            )
        )
    ]
    for one in loads:
        one.start()
    targets = []
    for sign in (1, -1):
        ok = (z + sign >= 0) & (z + sign < z_count)
        peer = ((z + sign + z_count) % z_count) * x_count + x
        targets.append((ok, peer))

    top[...] = jnp.full_like(top, -1e30)
    tot[...] = jnp.zeros_like(tot)
    acc[...] = jnp.zeros_like(acc)
    for one in loads:
        one.wait()

    bufs = (cb, kb, vb)

    def copies(src, way, peer):
        return [
            remote(b.at[src], b.at[src], send_sem.at[i, src, way], recv_sem.at[i, src], (peer, t))
            for i, b in enumerate(bufs)
        ]

    def source(k):
        low = jnp.minimum(z, z_count - 1 - z)
        both = k <= 2 * low
        dist = jnp.where(both, (k + 1) // 2, k - low)
        up = jnp.where(both, k % 2 == 1, z < z_count - 1 - z)
        return jnp.where(up, z + dist, z - dist)

    def update(i, keys, values_t, bias):
        sc = jnp.dot(keys, qt_ref[i], preferred_element_type=F32) * factor
        if bias != 0.0:
            sc = sc + bias
        old = top[i]
        new = jnp.maximum(old, jnp.max(sc, axis=0, keepdims=True))
        p = jnp.exp2(sc - new)
        f = jnp.exp2(old - new)
        top[i] = new
        tot[i] = tot[i] * f + jnp.sum(p, axis=0, keepdims=True)
        acc[i] = acc[i] * f + jnp.dot(values_t, p.astype(BF16), preferred_element_type=F32)

    def block(src):
        def head(i, carry):
            h = i // group
            update(i, kb[src, h], vb[src, h], 0.0)
            return carry

        lax.fori_loop(0, heads, head, 0)

    def wait_from(src):
        for one in copies(src, 0, s):
            one.wait_recv()

    def step(k, carry):
        zz = source(k)
        src = zz * x_count + x

        @pl.when(k > 0)
        def _():
            wait_from(src)

        for way, (ok, peer) in enumerate(targets):
            mine = zz <= z if way == 0 else zz >= z

            @pl.when(ok & mine)
            def _():
                for one in copies(src, way, peer):
                    one.start()

        for j in range(1, x_count):
            for one in copies(src, 1 + j, z * x_count + (x + j) % x_count):
                one.start()
        block(src)

        @pl.when(k > 0)
        def _():
            before = source(k - 1)
            for j in range(1, x_count):
                old = before * x_count + (x + j) % x_count
                wait_from(old)
                block(old)

        return carry

    lax.fori_loop(0, z_count, step, 0)
    final = source(z_count - 1)
    ends = [final * x_count + (x + j) % x_count for j in range(1, x_count)]
    for src in ends:
        copies(src, 0, s)[0].wait_recv()
    for i in range(heads):
        h = i // group
        keys = jnp.concatenate([cb[j, h, 0] for j in range(sp_count)], axis=0)
        vals = jnp.concatenate([cb[j, h, 1] for j in range(sp_count)], axis=0)
        update(i, keys, vals.astype(F32).T.astype(BF16), lift * math.log2(math.e))
    for src in ends:
        for one in copies(src, 0, s)[1:]:
            one.wait_recv()
        block(src)
    for i in range(heads):
        out_ref[:, i * head_dim : (i + 1) * head_dim] = (acc[i] / tot[i]).T.astype(BF16)

    def drain(k, carry):
        zz = source(k)
        src = zz * x_count + x
        for way, (ok, peer) in enumerate(targets):
            mine = zz <= z if way == 0 else zz >= z

            @pl.when(ok & mine)
            def _():
                for one in copies(src, way, peer):
                    one.wait_send()

        for j in range(1, x_count):
            for one in copies(src, 1 + j, z * x_count + (x + j) % x_count):
                one.wait_send()
        return carry

    lax.fori_loop(0, z_count, drain, 0)


def pair_kernel(
    sp_count, x_count, group, lift,
    k_hbm, vt_hbm, ckv_hbm, qt_ref,
    out_ref,
    kb, vb, cb, top, tot, acc, load_sem, qb, ab, send_sem, recv_sem, swap_sem,
):
    s, t = lax.axis_index("sp"), lax.axis_index("tp")
    z, x = s // x_count, s % x_count
    z_count = sp_count // x_count
    heads, head_dim, rows = qt_ref.shape
    factor = head_dim ** (-0.5) * math.log2(math.e)
    mine = z % 2
    mate = (z + 1 - 2 * mine) * x_count + x

    bufs = (cb, kb, vb)
    loads = [
        pltpu.make_async_copy(a, b.at[s], load_sem.at[i])
        for i, (a, b) in enumerate(zip((ckv_hbm, k_hbm, vt_hbm), bufs))
    ]
    for one in loads:
        one.start()
    swap_q = remote(
        qt_ref.at[pl.ds((1 - mine) * group, group)], qb.at[0],
        swap_sem.at[0], swap_sem.at[1], (mate, t),
    )
    swap_q.start()
    qb[1] = qt_ref[pl.ds(mine * group, group)]
    top[...] = jnp.full_like(top, -1e30)
    tot[...] = jnp.zeros_like(tot)
    acc[...] = jnp.zeros_like(acc)
    for one in loads:
        one.wait()

    def copy(i, src, h, way, peer):
        b = bufs[i]
        return remote(
            b.at[src, h], b.at[src, h], send_sem.at[i, way], recv_sem.at[i, src], (peer, t)
        )

    def source(k):
        low = jnp.minimum(z, z_count - 1 - z)
        both = k <= 2 * low
        dist = jnp.where(both, (k + 1) // 2, k - low)
        up = jnp.where(both, k % 2 == 1, z < z_count - 1 - z)
        return jnp.where(up, z + dist, z - dist)

    def line(act):
        for dist in range(1, z_count):
            for sign in (1, -1):
                there = z + sign * dist

                @pl.when((there >= 0) & (there < z_count))
                def _():
                    to = (there + z_count) % z_count
                    for i in range(3):
                        act(copy(i, s, to % 2, to, to * x_count + x))

    def across(k, act):
        zz = source(k)
        src = zz * x_count + x
        for i in range(3):
            if act is None:

                @pl.when(k > 0)
                def _():
                    copy(i, src, mine, 0, s).wait_recv()

            for j in range(1, x_count):
                way = z_count + zz * (x_count - 1) + j - 1
                one = copy(i, src, mine, way, z * x_count + (x + j) % x_count)
                one.start() if act is None else act(one)

    def update(i, queries, keys, values_t, bias):
        sc = jnp.dot(keys, queries, preferred_element_type=F32) * factor
        if bias != 0.0:
            sc = sc + bias
        old = top[i]
        new = jnp.maximum(old, jnp.max(sc, axis=0, keepdims=True))
        p = jnp.exp2(sc - new)
        f = jnp.exp2(old - new)
        top[i] = new
        tot[i] = tot[i] * f + jnp.sum(p, axis=0, keepdims=True)
        acc[i] = acc[i] * f + jnp.dot(values_t, p.astype(BF16), preferred_element_type=F32)

    def block(src):
        def tile(i, carry):
            update(i, qb[i // group, i % group], kb[src, mine], vb[src, mine], 0.0)
            return carry

        lax.fori_loop(0, 2 * group, tile, 0)

    def step(k, carry):
        across(k, None)

        @pl.when(k == 0)
        def _():
            swap_q.wait_recv()

        block(source(k) * x_count + x)

        @pl.when(k > 0)
        def _():
            before = source(k - 1)
            for j in range(1, x_count):
                old = before * x_count + (x + j) % x_count
                for i in range(3):
                    copy(i, old, mine, 0, s).wait_recv()
                block(old)

        return carry

    line(lambda one: one.start())
    lax.fori_loop(0, z_count, step, 0)
    final = source(z_count - 1)
    ends = [final * x_count + (x + j) % x_count for j in range(1, x_count)]
    for src in ends:
        copy(0, src, mine, 0, s).wait_recv()
    keys = jnp.concatenate([cb[j, mine, 0] for j in range(sp_count)], axis=0)
    vals = jnp.concatenate([cb[j, mine, 1] for j in range(sp_count)], axis=0)
    vals = vals.astype(F32).T.astype(BF16)
    span = group * head_dim
    swap_a = remote(ab.at[0], ab.at[1], swap_sem.at[2], swap_sem.at[3], (mate, t))
    for who in range(2):
        for g in range(group):
            update(who * group + g, qb[who, g], keys, vals, lift * math.log2(math.e))
        for src in ends:
            if who == 0:
                for i in (1, 2):
                    copy(i, src, mine, 0, s).wait_recv()
            for g in range(group):
                update(who * group + g, qb[who, g], kb[src, mine], vb[src, mine], 0.0)
        for g in range(group):
            i = who * group + g
            done = (acc[i] / tot[i]).T.astype(BF16)
            if who == 0:
                ab[0, :, g * head_dim : (g + 1) * head_dim] = done
            else:
                at = pl.ds(pl.multiple_of(mine * span + g * head_dim, head_dim), head_dim)
                out_ref[:, at] = done
        if who == 0:
            swap_a.start()

    def drain(k, carry):
        across(k, lambda one: one.wait_send())
        return carry

    lax.fori_loop(0, z_count, drain, 0)
    line(lambda one: one.wait_send())
    swap_a.wait_recv()
    out_ref[:, pl.ds(pl.multiple_of((1 - mine) * span, head_dim), span)] = ab[1]
    swap_q.wait_send()
    swap_a.wait_send()


def mix_kernel(
    tp_count, chunks,
    att_ref, wo_hbm, wo_ref, wo_sem, lat_ref, gate_ref,
    out_ref,
    core_out, core_in, mesh_out, mesh_in, mixed, core_send, core_recv, mesh_send, mesh_recv,
):
    s, t = lax.axis_index("sp"), lax.axis_index("tp")
    y, c = t // 2, t % 2
    y_count = tp_count // 2
    partner = y * 2 + 1 - c
    rows, width = lat_ref.shape
    step = width // chunks
    peers = [((y + j) % y_count) * 2 + c for j in range(1, y_count)]
    pltpu.make_async_copy(wo_hbm, wo_ref, wo_sem.at[0]).wait()

    def piece(n, j, cc):
        yy = (y + j) % y_count
        at = pl.ds(pl.multiple_of((yy * 2 + cc) * rows, rows), rows)
        return jnp.dot(
            att_ref[at, :], wo_ref[:, n * step : (n + 1) * step], preferred_element_type=F32
        )

    order = list(range(1, y_count)) + [0]
    cores = [
        remote(core_out.at[n], core_in.at[n], core_send.at[n], core_recv.at[n], (s, partner))
        for n in range(chunks)
    ]
    sent = []
    for n in range(chunks):
        for j in order:
            core_out[n, j] = piece(n, j, 1 - c).astype(BF16)
        cores[n].start()
    for n in range(chunks):
        mine = [piece(n, j, c) for j in order]
        cores[n].wait_recv()
        for j, value in zip(order, mine):
            value = value + core_in[n, j].astype(F32)
            if j == 0:
                mixed[n] = value
            else:
                mesh_out[n, j - 1] = value.astype(BF16)
                one = remote(
                    mesh_out.at[n, j - 1], mesh_in.at[n, j - 1], mesh_send.at[n, j - 1],
                    mesh_recv.at[n, j - 1], (s, peers[j - 1]),
                )
                one.start()
                sent.append(one)
    for one in sent:
        one.wait_recv()
    square = jnp.zeros((rows, 1), F32)
    for n in range(chunks):
        value = mixed[n]
        for j in range(1, y_count):
            value = value + mesh_in[n, j - 1].astype(F32)
        mixed[n] = value
        square = square + jnp.sum(value * value, axis=-1, keepdims=True)
    inv = lax.rsqrt(square / width + NORM_EPS)
    for n in range(chunks):
        at = slice(n * step, (n + 1) * step)
        out_ref[:, at] = (
            lat_ref[:, at].astype(F32) + gate_ref[:, at] * (mixed[n] * inv)
        ).astype(BF16)
    for one in sent + cores:
        one.wait_send()


def whole_kernel(sp_count, tp_count, x_count, head_dim, group, lift, chunks, paired, counts, *refs):
    (
        cond, mw, lat, ctx, wq, wk, wv, qg, kg, cos, sin, wo, lat_rows,
        out, qt, k, vt, ckv, gate, att, wo_vm, wo_sem, *rest,
    ) = refs
    front, middle, last = counts
    front_scratch, middle_scratch = rest[:front], rest[front : front + middle]
    front_kernel(
        sp_count, tp_count, head_dim, cond, mw, lat, ctx, wq, wk, wv, qg, kg, cos, sin,
        qt, k, vt, ckv, gate, *front_scratch, wo, wo_vm, wo_sem,
    )
    attention = pair_kernel if paired else attend_kernel
    attention(sp_count, x_count, group, lift, k, vt, ckv, qt, att, *middle_scratch)
    mix_kernel(
        tp_count, chunks, att, wo, wo_vm, wo_sem, lat_rows, gate, out, *rest[front + middle :]
    )


ANY = pl.BlockSpec(memory_space=pl.ANY)
VM = pl.BlockSpec(memory_space=pltpu.VMEM)
DMA = pltpu.SemaphoreType.DMA


def body(
    latents,
    context,
    cond,
    ctx_cond,
    mod_weight,
    query_weight,
    key_matrix,
    value_matrix,
    out_weight,
    query_gain,
    key_gain,
):
    sp_count, tp_count = lax.axis_size("sp"), lax.axis_size("tp")
    x_count = row_size(sp_count)
    rows, width = latents.shape
    ctx_rows = context.shape[0]
    head_dim = query_gain.shape[0]
    heads = query_weight.shape[1] // head_dim
    kv_heads = key_matrix.shape[1] // head_dim
    all_rows = rows * tp_count
    mod_cols = mod_weight.shape[1]
    positions = lax.axis_index("sp") * all_rows + jnp.arange(all_rows, dtype=jnp.int32)
    cos, sin = tables(positions, head_dim)
    pair = jnp.concatenate(
        [cond[None], ctx_cond[None], jnp.zeros((6, cond.shape[0]), F32)], axis=0
    )
    sds = jax.ShapeDtypeStruct
    lift = math.log(sp_count * all_rows / (2.0 * sp_count * ctx_rows))
    group = heads // kv_heads
    paired = kv_heads == 2 and (sp_count // x_count) % 2 == 0
    chunks = 4
    y_count = tp_count // 2
    step = width // chunks
    far = max(y_count - 1, 1)
    shared = [
        pltpu.VMEM((heads, head_dim, all_rows), BF16),
        pltpu.VMEM((kv_heads, all_rows, head_dim), BF16),
        pltpu.VMEM((kv_heads, head_dim, all_rows), BF16),
        pltpu.VMEM((kv_heads, 2, ctx_rows, head_dim), BF16),
        pltpu.VMEM((1, width), F32),
        pltpu.VMEM((all_rows, heads * head_dim), BF16),
        pltpu.VMEM(out_weight.shape, BF16),
        DMA((1,)),
    ]
    front = [
        pltpu.VMEM(mod_weight.shape, F32),
        pltpu.VMEM((tp_count, rows, width), BF16),
        pltpu.VMEM(query_weight.shape, BF16),
        pltpu.VMEM(key_matrix.shape, BF16),
        pltpu.VMEM(value_matrix.shape, BF16),
        pltpu.VMEM((sp_count, 2, mod_cols), F32),
        pltpu.VMEM((tp_count, 2, mod_cols), F32),
        pltpu.VMEM((2, mod_cols * tp_count), F32),
        pltpu.VMEM((2 * rows, width), BF16),
        DMA((5,)),
        DMA((tp_count,)),
        DMA((tp_count,)),
        DMA((sp_count,)),
        DMA((sp_count,)),
        DMA((tp_count,)),
        DMA((tp_count,)),
    ]
    middle = [
        pltpu.VMEM((sp_count, kv_heads, all_rows, head_dim), BF16),
        pltpu.VMEM((sp_count, kv_heads, head_dim, all_rows), BF16),
        pltpu.VMEM((sp_count, kv_heads, 2, ctx_rows, head_dim), BF16),
        pltpu.VMEM((heads, 1, all_rows), F32),
        pltpu.VMEM((heads, 1, all_rows), F32),
        pltpu.VMEM((heads, head_dim, all_rows), F32),
        DMA((3,)),
    ]
    if paired:
        middle += [
            pltpu.VMEM((2, group, head_dim, all_rows), BF16),
            pltpu.VMEM((2, all_rows, group * head_dim), BF16),
            DMA((3, sp_count)),
            DMA((3, sp_count)),
            DMA((4,)),
        ]
    else:
        middle += [DMA((3, sp_count, x_count + 1)), DMA((3, sp_count))]
    last = [
        pltpu.VMEM((chunks, y_count, rows, step), BF16),
        pltpu.VMEM((chunks, y_count, rows, step), BF16),
        pltpu.VMEM((chunks, far, rows, step), BF16),
        pltpu.VMEM((chunks, far, rows, step), BF16),
        pltpu.VMEM((chunks, rows, step), F32),
        DMA((chunks,)),
        DMA((chunks,)),
        DMA((chunks, far)),
        DMA((chunks, far)),
    ]
    counts = (len(front), len(middle), len(last))
    return pl.pallas_call(
        functools.partial(
            whole_kernel, sp_count, tp_count, x_count, head_dim, group, lift, chunks, paired, counts
        ),
        out_shape=jax.ShapeDtypeStruct((rows, width), BF16),
        in_specs=[VM, ANY, ANY, VM, ANY, ANY, ANY, VM, VM, VM, VM, ANY, VM],
        out_specs=VM,
        scratch_shapes=shared + front + middle + last,
        compiler_params=pltpu.CompilerParams(
            collective_id=0, has_side_effects=True, vmem_limit_bytes=VMEM_BYTES
        ),
        name="whole",
    )(
        pair, mod_weight, latents, context, query_weight, key_matrix, value_matrix,
        query_gain[None], key_gain[None], cos, sin, out_weight, latents,
    )


def solution(mesh):
    placed = (
        P(("sp", "tp"), None),
        P("sp", None),
        P("sp"),
        P("sp"),
        P("sp", "tp"),
        P(None, "tp"),
        P(None, "tp"),
        P(None, "tp"),
        P("tp", None),
        P(),
        P(),
    )
    return jax.shard_map(
        body, mesh=mesh, in_specs=placed, out_specs=P(("sp", "tp"), None), check_vma=False
    )
```

```python
import functools
import math

import jax
import jax.numpy as jnp
from jax import lax
from jax.experimental import pallas as pl
from jax.experimental.pallas import tpu as pltpu
from jax.sharding import PartitionSpec as P

GRID_W = 64
NORM_EPS = 1e-06
ROPE_BASE = 10000.0
MESH = pl.DeviceIdType.MESH
BF16 = jnp.bfloat16
F32 = jnp.float32
VMEM_BYTES = 67043328


def row_size(sp_count):
    size = 1
    while 4 * size * size <= sp_count:
        size *= 2
    return size


def tables(positions, head_dim):
    quarter = head_dim // 4
    inv_freq = ROPE_BASE ** (-jnp.arange(quarter, dtype=F32) / quarter)
    where = jnp.stack([positions // GRID_W, positions % GRID_W]).astype(F32)
    angles = where[:, None, :] * inv_freq[None, :, None]
    return jnp.cos(angles), jnp.sin(angles)


def remote(src, dst, send, recv, dev):
    return pltpu.make_async_remote_copy(
        src_ref=src, dst_ref=dst, send_sem=send, recv_sem=recv, device_id=dev, device_id_type=MESH
    )


def front_kernel(
    sp_count, tp_count, head_dim,
    cond_ref, cond_1_ref, mw_hbm, lat_hbm, ctx_ref, wq_hbm, wk_hbm, wv_hbm, qg_ref, kg_ref, cos_ref, sin_ref,
    qt_ref, k_ref, vt_ref, ckv_ref, gate_ref,
    mw, lat, wq, wk, wv, part, tot, mod, xn, load_sem,
    lat_send, lat_recv, part_send, part_recv, tot_send, tot_recv,
    wo_hbm, wo_vm, wo_sem,
):
    s, t = lax.axis_index("sp"), lax.axis_index("tp")
    y, c = t // 2, t % 2
    y_count = tp_count // 2
    partner = y * 2 + 1 - c
    rows = lat.shape[1]
    width = lat.shape[2]
    model_cols = mod.shape[1]

    own = pltpu.make_async_copy(lat_hbm, lat.at[t], load_sem.at[0])
    own.start()
    loads = [
        pltpu.make_async_copy(a, b, load_sem.at[1 + i])
        for i, (a, b) in enumerate(((mw_hbm, mw), (wq_hbm, wq), (wk_hbm, wk), (wv_hbm, wv)))
    ]
    for one in loads:
        one.start()

    pltpu.make_async_copy(wo_hbm, wo_vm, wo_sem.at[0]).start()

    barrier = pltpu.get_barrier_semaphore()
    for j in range(1, sp_count):
        pl.semaphore_signal(barrier, inc=1, device_id=((s + j) % sp_count, t), device_id_type=MESH)
    for j in range(1, tp_count):
        pl.semaphore_signal(barrier, inc=1, device_id=(s, (t + j) % tp_count), device_id_type=MESH)
    pl.semaphore_wait(barrier, sp_count + tp_count - 2)

    own.wait()
    sends = []
    for j in range(1, y_count):
        peer = ((y + j) % y_count) * 2 + c
        sends.append(remote(lat.at[t], lat.at[t], lat_send.at[j], lat_recv.at[t], (s, peer)))
    sends.append(remote(lat.at[t], lat.at[t], lat_send.at[0], lat_recv.at[t], (s, partner)))
    for one in sends:
        one.start()

    loads[0].wait()
    lines = lax.broadcasted_iota(jnp.int32, (8, cond_ref.shape[1]), 0)
    cond = jnp.where(lines == 0, cond_ref[...], jnp.where(lines == 1, cond_1_ref[...], 0.0))
    cond = cond * jax.nn.sigmoid(cond)
    part[s] = jnp.dot(
        cond, mw[...], precision=lax.Precision.HIGHEST, preferred_element_type=F32
    )[:2]
    more = [
        remote(part.at[s], part.at[s], part_send.at[j], part_recv.at[s], ((s + j) % sp_count, t))
        for j in range(1, sp_count)
    ]
    for one in more:
        one.start()
    for j in range(1, sp_count):
        src = (s + j) % sp_count
        remote(part.at[src], part.at[src], part_send.at[0], part_recv.at[src], (s, t)).wait_recv()
    total = part[0]
    for j in range(1, sp_count):
        total = total + part[j]
    tot[t] = total
    last = [
        remote(tot.at[t], tot.at[t], tot_send.at[j], tot_recv.at[t], (s, (t + j) % tp_count))
        for j in range(1, tp_count)
    ]
    for one in last:
        one.start()
    for j in range(1, tp_count):
        src = (t + j) % tp_count
        remote(tot.at[src], tot.at[src], tot_send.at[0], tot_recv.at[src], (s, t)).wait_recv()
    cols = model_cols // tp_count
    for j in range(tp_count):
        mod[:, j * cols : (j + 1) * cols] = tot[j]
    gate_ref[...] = mod[0:1, 2 * width :]

    def modulate(x, r):
        x = x.astype(F32)
        scaled = x * lax.rsqrt(jnp.mean(x * x, axis=-1, keepdims=True) + NORM_EPS)
        shift, scale = mod[r : r + 1, :width], mod[r : r + 1, width : 2 * width]
        return (scaled * (1.0 + scale) + shift).astype(BF16)

    for one in loads[1:]:
        one.wait()

    cn = modulate(ctx_ref[...], 1)
    kc = jnp.dot(cn, wk[...], preferred_element_type=F32)
    vc = jnp.dot(cn, wv[...], preferred_element_type=F32)
    for h in range(kc.shape[1] // head_dim):
        kh = kc[:, h * head_dim : (h + 1) * head_dim]
        kh = kh * lax.rsqrt(jnp.mean(kh * kh, axis=-1, keepdims=True) + NORM_EPS) * kg_ref[...]
        ckv_ref[h, 0] = kh.astype(BF16)
        ckv_ref[h, 1] = vc[:, h * head_dim : (h + 1) * head_dim].astype(BF16)

    q4 = head_dim // 4
    qgain, kgain = qg_ref[...], kg_ref[...]

    def turn(yt, cos, sin):
        out = []
        for n in range(2):
            a = yt[2 * n * q4 : (2 * n + 1) * q4]
            b = yt[(2 * n + 1) * q4 : (2 * n + 2) * q4]
            out += [a * cos[n] - b * sin[n], b * cos[n] + a * sin[n]]
        return jnp.concatenate(out, axis=0)

    def unit(yh, gain):
        return yh * lax.rsqrt(jnp.mean(yh * yh, axis=-1, keepdims=True) + NORM_EPS) * gain

    span = 2 * rows
    relays = []
    for j in range(y_count):
        yy = (y + j) % y_count
        if j > 0:
            src = yy * 2 + c
            remote(lat.at[src], lat.at[src], lat_send.at[0], lat_recv.at[src], (s, t)).wait_recv()
            one = remote(
                lat.at[src], lat.at[src], lat_send.at[y_count - 1 + j], lat_recv.at[src], (s, partner)
            )
            one.start()
            relays.append(one)
        other = yy * 2 + 1 - c
        remote(lat.at[other], lat.at[other], lat_send.at[0], lat_recv.at[other], (s, t)).wait_recv()
        for i in range(2):
            xn[i * rows : (i + 1) * rows, :] = modulate(lat[yy * 2 + i], 0)
        x = xn[...]
        at = pl.ds(pl.multiple_of(yy * span, span), span)
        cos, sin = cos_ref[:, :, at], sin_ref[:, :, at]
        for w, kind in ((wq, 0), (wk, 1), (wv, 2)):
            step = min(2 * head_dim, w.shape[1])
            for n in range(0, w.shape[1], step):
                full = jnp.dot(x, w[:, n : n + step], preferred_element_type=F32)
                for m in range(0, step, head_dim):
                    h = (n + m) // head_dim
                    yh = full[:, m : m + head_dim]
                    if kind == 0:
                        qt_ref[h, :, at] = turn(unit(yh, qgain).T, cos, sin).astype(BF16)
                    elif kind == 1:
                        k_ref[h, at, :] = turn(unit(yh, kgain).T, cos, sin).T.astype(BF16)
                    else:
                        vt_ref[h, :, at] = yh.T.astype(BF16)
    for one in sends + more + last + relays:
        one.wait_send()


def attend_kernel(
    sp_count, x_count, group, lift,
    k_hbm, vt_hbm, ckv_hbm, qt_ref,
    out_ref,
    kb, vb, cb, top, tot, acc, load_sem, send_sem, recv_sem,
):
    s, t = lax.axis_index("sp"), lax.axis_index("tp")
    z, x = s // x_count, s % x_count
    z_count = sp_count // x_count
    heads, head_dim, rows = qt_ref.shape
    kv_heads = heads // group
    factor = head_dim ** (-0.5) * math.log2(math.e)

    loads = [
        pltpu.make_async_copy(a, b, load_sem.at[i])
        for i, (a, b) in enumerate(
            (
                (ckv_hbm, cb.at[s]),
                (k_hbm, kb.at[s]),
                (vt_hbm, vb.at[s]),
            )
        )
    ]
    for one in loads:
        one.start()
    targets = []
    for sign in (1, -1):
        ok = (z + sign >= 0) & (z + sign < z_count)
        peer = ((z + sign + z_count) % z_count) * x_count + x
        targets.append((ok, peer))

    top[...] = jnp.full_like(top, -1e30)
    tot[...] = jnp.zeros_like(tot)
    acc[...] = jnp.zeros_like(acc)
    for one in loads:
        one.wait()

    bufs = (cb, kb, vb)

    def copies(src, way, peer):
        return [
            remote(b.at[src], b.at[src], send_sem.at[i, src, way], recv_sem.at[i, src], (peer, t))
            for i, b in enumerate(bufs)
        ]

    def source(k):
        low = jnp.minimum(z, z_count - 1 - z)
        both = k <= 2 * low
        dist = jnp.where(both, (k + 1) // 2, k - low)
        up = jnp.where(both, k % 2 == 1, z < z_count - 1 - z)
        return jnp.where(up, z + dist, z - dist)

    def update(i, keys, values_t, bias):
        sc = jnp.dot(keys, qt_ref[i], preferred_element_type=F32) * factor
        if bias != 0.0:
            sc = sc + bias
        old = top[i]
        new = jnp.maximum(old, jnp.max(sc, axis=0, keepdims=True))
        p = jnp.exp2(sc - new)
        f = jnp.exp2(old - new)
        top[i] = new
        tot[i] = tot[i] * f + jnp.sum(p, axis=0, keepdims=True)
        acc[i] = acc[i] * f + jnp.dot(values_t, p.astype(BF16), preferred_element_type=F32)

    def block(src):
        def head(i, carry):
            h = i // group
            update(i, kb[src, h], vb[src, h], 0.0)
            return carry

        lax.fori_loop(0, heads, head, 0)

    def wait_from(src):
        for one in copies(src, 0, s):
            one.wait_recv()

    def step(k, carry):
        zz = source(k)
        src = zz * x_count + x

        @pl.when(k > 0)
        def _():
            wait_from(src)

        for way, (ok, peer) in enumerate(targets):
            mine = zz <= z if way == 0 else zz >= z

            @pl.when(ok & mine)
            def _():
                for one in copies(src, way, peer):
                    one.start()

        for j in range(1, x_count):
            for one in copies(src, 1 + j, z * x_count + (x + j) % x_count):
                one.start()
        block(src)

        @pl.when(k > 0)
        def _():
            before = source(k - 1)
            for j in range(1, x_count):
                old = before * x_count + (x + j) % x_count
                wait_from(old)
                block(old)

        return carry

    lax.fori_loop(0, z_count, step, 0)
    final = source(z_count - 1)
    ends = [final * x_count + (x + j) % x_count for j in range(1, x_count)]
    for src in ends:
        copies(src, 0, s)[0].wait_recv()
    for i in range(heads):
        h = i // group
        keys = jnp.concatenate([cb[j, h, 0] for j in range(sp_count)], axis=0)
        vals = jnp.concatenate([cb[j, h, 1] for j in range(sp_count)], axis=0)
        update(i, keys, vals.astype(F32).T.astype(BF16), lift * math.log2(math.e))
    for src in ends:
        for one in copies(src, 0, s)[1:]:
            one.wait_recv()
        block(src)
    for i in range(heads):
        out_ref[:, i * head_dim : (i + 1) * head_dim] = (acc[i] / tot[i]).T.astype(BF16)

    def drain(k, carry):
        zz = source(k)
        src = zz * x_count + x
        for way, (ok, peer) in enumerate(targets):
            mine = zz <= z if way == 0 else zz >= z

            @pl.when(ok & mine)
            def _():
                for one in copies(src, way, peer):
                    one.wait_send()

        for j in range(1, x_count):
            for one in copies(src, 1 + j, z * x_count + (x + j) % x_count):
                one.wait_send()
        return carry

    lax.fori_loop(0, z_count, drain, 0)


def pair_kernel(
    sp_count, x_count, group, lift,
    k_hbm, vt_hbm, ckv_hbm, qt_ref,
    out_ref,
    kb, vb, cb, top, tot, acc, load_sem, qb, ab, send_sem, recv_sem, swap_sem,
):
    s, t = lax.axis_index("sp"), lax.axis_index("tp")
    z, x = s // x_count, s % x_count
    z_count = sp_count // x_count
    heads, head_dim, rows = qt_ref.shape
    factor = head_dim ** (-0.5) * math.log2(math.e)
    mine = z % 2
    mate = (z + 1 - 2 * mine) * x_count + x

    bufs = (cb, kb, vb)
    loads = [
        pltpu.make_async_copy(a, b.at[s], load_sem.at[i])
        for i, (a, b) in enumerate(zip((ckv_hbm, k_hbm, vt_hbm), bufs))
    ]
    for one in loads:
        one.start()
    swap_q = remote(
        qt_ref.at[pl.ds((1 - mine) * group, group)], qb.at[0],
        swap_sem.at[0], swap_sem.at[1], (mate, t),
    )
    swap_q.start()
    qb[1] = qt_ref[pl.ds(mine * group, group)]
    top[...] = jnp.full_like(top, -1e30)
    tot[...] = jnp.zeros_like(tot)
    acc[...] = jnp.zeros_like(acc)
    for one in loads:
        one.wait()

    def copy(i, src, h, way, peer):
        b = bufs[i]
        return remote(
            b.at[src, h], b.at[src, h], send_sem.at[i, way], recv_sem.at[i, src], (peer, t)
        )

    def source(k):
        low = jnp.minimum(z, z_count - 1 - z)
        both = k <= 2 * low
        dist = jnp.where(both, (k + 1) // 2, k - low)
        up = jnp.where(both, k % 2 == 1, z < z_count - 1 - z)
        return jnp.where(up, z + dist, z - dist)

    def line(act):
        for dist in range(1, z_count):
            for sign in (1, -1):
                there = z + sign * dist

                @pl.when((there >= 0) & (there < z_count))
                def _():
                    to = (there + z_count) % z_count
                    for i in range(3):
                        act(copy(i, s, to % 2, to, to * x_count + x))

    def across(k, act):
        zz = source(k)
        src = zz * x_count + x
        for i in range(3):
            if act is None:

                @pl.when(k > 0)
                def _():
                    copy(i, src, mine, 0, s).wait_recv()

            for j in range(1, x_count):
                way = z_count + zz * (x_count - 1) + j - 1
                one = copy(i, src, mine, way, z * x_count + (x + j) % x_count)
                one.start() if act is None else act(one)

    def update(i, queries, keys, values_t, bias):
        sc = jnp.dot(keys, queries, preferred_element_type=F32) * factor
        if bias != 0.0:
            sc = sc + bias
        old = top[i]
        new = jnp.maximum(old, jnp.max(sc, axis=0, keepdims=True))
        p = jnp.exp2(sc - new)
        f = jnp.exp2(old - new)
        top[i] = new
        tot[i] = tot[i] * f + jnp.sum(p, axis=0, keepdims=True)
        acc[i] = acc[i] * f + jnp.dot(values_t, p.astype(BF16), preferred_element_type=F32)

    def block(src):
        def tile(i, carry):
            update(i, qb[i // group, i % group], kb[src, mine], vb[src, mine], 0.0)
            return carry

        lax.fori_loop(0, 2 * group, tile, 0)

    def step(k, carry):
        across(k, None)

        @pl.when(k == 0)
        def _():
            swap_q.wait_recv()

        block(source(k) * x_count + x)

        @pl.when(k > 0)
        def _():
            before = source(k - 1)
            for j in range(1, x_count):
                old = before * x_count + (x + j) % x_count
                for i in range(3):
                    copy(i, old, mine, 0, s).wait_recv()
                block(old)

        return carry

    line(lambda one: one.start())
    lax.fori_loop(0, z_count, step, 0)
    final = source(z_count - 1)
    ends = [final * x_count + (x + j) % x_count for j in range(1, x_count)]
    for src in ends:
        copy(0, src, mine, 0, s).wait_recv()
    keys = jnp.concatenate([cb[j, mine, 0] for j in range(sp_count)], axis=0)
    vals = jnp.concatenate([cb[j, mine, 1] for j in range(sp_count)], axis=0)
    vals = vals.astype(F32).T.astype(BF16)
    span = group * head_dim
    swap_a = remote(ab.at[0], ab.at[1], swap_sem.at[2], swap_sem.at[3], (mate, t))
    for who in range(2):
        for g in range(group):
            update(who * group + g, qb[who, g], keys, vals, lift * math.log2(math.e))
        for src in ends:
            if who == 0:
                for i in (1, 2):
                    copy(i, src, mine, 0, s).wait_recv()
            for g in range(group):
                update(who * group + g, qb[who, g], kb[src, mine], vb[src, mine], 0.0)
        for g in range(group):
            i = who * group + g
            done = (acc[i] / tot[i]).T.astype(BF16)
            if who == 0:
                ab[0, :, g * head_dim : (g + 1) * head_dim] = done
            else:
                at = pl.ds(pl.multiple_of(mine * span + g * head_dim, head_dim), head_dim)
                out_ref[:, at] = done
        if who == 0:
            swap_a.start()

    def drain(k, carry):
        across(k, lambda one: one.wait_send())
        return carry

    lax.fori_loop(0, z_count, drain, 0)
    line(lambda one: one.wait_send())
    swap_a.wait_recv()
    out_ref[:, pl.ds(pl.multiple_of((1 - mine) * span, head_dim), span)] = ab[1]
    swap_q.wait_send()
    swap_a.wait_send()


def mix_kernel(
    tp_count, chunks,
    att_ref, wo_hbm, wo_ref, wo_sem, lat_ref, gate_ref,
    out_ref,
    core_out, core_in, mesh_out, mesh_in, mixed, core_send, core_recv, mesh_send, mesh_recv,
):
    s, t = lax.axis_index("sp"), lax.axis_index("tp")
    y, c = t // 2, t % 2
    y_count = tp_count // 2
    partner = y * 2 + 1 - c
    rows, width = lat_ref.shape
    step = width // chunks
    peers = [((y + j) % y_count) * 2 + c for j in range(1, y_count)]
    pltpu.make_async_copy(wo_hbm, wo_ref, wo_sem.at[0]).wait()

    def piece(n, j, cc):
        yy = (y + j) % y_count
        at = pl.ds(pl.multiple_of((yy * 2 + cc) * rows, rows), rows)
        return jnp.dot(
            att_ref[at, :], wo_ref[:, n * step : (n + 1) * step], preferred_element_type=F32
        )

    order = list(range(1, y_count)) + [0]
    cores = [
        remote(core_out.at[n], core_in.at[n], core_send.at[n], core_recv.at[n], (s, partner))
        for n in range(chunks)
    ]
    sent = []
    for n in range(chunks + 1):
        if n < chunks:
            for j in order:
                core_out[n, j] = piece(n, j, 1 - c).astype(BF16)
            cores[n].start()
        if n == 0:
            continue
        m = n - 1
        own = [piece(m, j, c) for j in order]
        cores[m].wait_recv()
        for j, value in zip(order, own):
            value = value + core_in[m, j].astype(F32)
            if j == 0:
                mixed[m] = value
            else:
                mesh_out[m, j - 1] = value.astype(BF16)
                one = remote(
                    mesh_out.at[m, j - 1], mesh_in.at[m, j - 1], mesh_send.at[m, j - 1],
                    mesh_recv.at[m, j - 1], (s, peers[j - 1]),
                )
                one.start()
                sent.append(one)
    for one in sent:
        one.wait_recv()
    square = jnp.zeros((rows, 1), F32)
    for n in range(chunks):
        value = mixed[n]
        for j in range(1, y_count):
            value = value + mesh_in[n, j - 1].astype(F32)
        mixed[n] = value
        square = square + jnp.sum(value * value, axis=-1, keepdims=True)
    inv = lax.rsqrt(square / width + NORM_EPS)
    for n in range(chunks):
        at = slice(n * step, (n + 1) * step)
        out_ref[:, at] = (
            lat_ref[:, at].astype(F32) + gate_ref[:, at] * (mixed[n] * inv)
        ).astype(BF16)
    for one in sent + cores:
        one.wait_send()


def whole_kernel(sp_count, tp_count, x_count, head_dim, group, lift, chunks, paired, counts, *refs):
    (
        cond, cond_1, mw, lat, ctx, wq, wk, wv, qg, kg, cos, sin, wo, lat_rows,
        out, qt, k, vt, ckv, gate, att, wo_vm, wo_sem, *rest,
    ) = refs
    front, middle, last = counts
    front_scratch, middle_scratch = rest[:front], rest[front : front + middle]
    front_kernel(
        sp_count, tp_count, head_dim, cond, cond_1, mw, lat, ctx, wq, wk, wv, qg, kg, cos, sin,
        qt, k, vt, ckv, gate, *front_scratch, wo, wo_vm, wo_sem,
    )
    attention = pair_kernel if paired else attend_kernel
    attention(sp_count, x_count, group, lift, k, vt, ckv, qt, att, *middle_scratch)
    mix_kernel(
        tp_count, chunks, att, wo, wo_vm, wo_sem, lat_rows, gate, out, *rest[front + middle :]
    )


ANY = pl.BlockSpec(memory_space=pl.ANY)
VM = pl.BlockSpec(memory_space=pltpu.VMEM)
DMA = pltpu.SemaphoreType.DMA


def body(
    latents,
    context,
    cond,
    ctx_cond,
    mod_weight,
    query_weight,
    key_matrix,
    value_matrix,
    out_weight,
    query_gain,
    key_gain,
):
    sp_count, tp_count = lax.axis_size("sp"), lax.axis_size("tp")
    x_count = row_size(sp_count)
    rows, width = latents.shape
    ctx_rows = context.shape[0]
    head_dim = query_gain.shape[0]
    heads = query_weight.shape[1] // head_dim
    kv_heads = key_matrix.shape[1] // head_dim
    all_rows = rows * tp_count
    mod_cols = mod_weight.shape[1]
    positions = lax.axis_index("sp") * all_rows + jnp.arange(all_rows, dtype=jnp.int32)
    cos, sin = tables(positions, head_dim)
    lift = math.log(sp_count * all_rows / (2.0 * sp_count * ctx_rows))
    group = heads // kv_heads
    paired = kv_heads == 2 and (sp_count // x_count) % 2 == 0
    chunks = 4
    y_count = tp_count // 2
    step = width // chunks
    far = max(y_count - 1, 1)
    shared = [
        pltpu.VMEM((heads, head_dim, all_rows), BF16),
        pltpu.VMEM((kv_heads, all_rows, head_dim), BF16),
        pltpu.VMEM((kv_heads, head_dim, all_rows), BF16),
        pltpu.VMEM((kv_heads, 2, ctx_rows, head_dim), BF16),
        pltpu.VMEM((1, width), F32),
        pltpu.VMEM((all_rows, heads * head_dim), BF16),
        pltpu.VMEM(out_weight.shape, BF16),
        DMA((1,)),
    ]
    front = [
        pltpu.VMEM(mod_weight.shape, F32),
        pltpu.VMEM((tp_count, rows, width), BF16),
        pltpu.VMEM(query_weight.shape, BF16),
        pltpu.VMEM(key_matrix.shape, BF16),
        pltpu.VMEM(value_matrix.shape, BF16),
        pltpu.VMEM((sp_count, 2, mod_cols), F32),
        pltpu.VMEM((tp_count, 2, mod_cols), F32),
        pltpu.VMEM((2, mod_cols * tp_count), F32),
        pltpu.VMEM((2 * rows, width), BF16),
        DMA((5,)),
        DMA((tp_count,)),
        DMA((tp_count,)),
        DMA((sp_count,)),
        DMA((sp_count,)),
        DMA((tp_count,)),
        DMA((tp_count,)),
    ]
    middle = [
        pltpu.VMEM((sp_count, kv_heads, all_rows, head_dim), BF16),
        pltpu.VMEM((sp_count, kv_heads, head_dim, all_rows), BF16),
        pltpu.VMEM((sp_count, kv_heads, 2, ctx_rows, head_dim), BF16),
        pltpu.VMEM((heads, 1, all_rows), F32),
        pltpu.VMEM((heads, 1, all_rows), F32),
        pltpu.VMEM((heads, head_dim, all_rows), F32),
        DMA((3,)),
    ]
    if paired:
        middle += [
            pltpu.VMEM((2, group, head_dim, all_rows), BF16),
            pltpu.VMEM((2, all_rows, group * head_dim), BF16),
            DMA((3, sp_count)),
            DMA((3, sp_count)),
            DMA((4,)),
        ]
    else:
        middle += [DMA((3, sp_count, x_count + 1)), DMA((3, sp_count))]
    last = [
        pltpu.VMEM((chunks, y_count, rows, step), BF16),
        pltpu.VMEM((chunks, y_count, rows, step), BF16),
        pltpu.VMEM((chunks, far, rows, step), BF16),
        pltpu.VMEM((chunks, far, rows, step), BF16),
        pltpu.VMEM((chunks, rows, step), F32),
        DMA((chunks,)),
        DMA((chunks,)),
        DMA((chunks, far)),
        DMA((chunks, far)),
    ]
    counts = (len(front), len(middle), len(last))
    return pl.pallas_call(
        functools.partial(
            whole_kernel, sp_count, tp_count, x_count, head_dim, group, lift, chunks, paired, counts
        ),
        out_shape=jax.ShapeDtypeStruct((rows, width), BF16),
        in_specs=[VM, VM, ANY, ANY, VM, ANY, ANY, ANY, VM, VM, VM, VM, ANY, VM],
        out_specs=VM,
        scratch_shapes=shared + front + middle + last,
        compiler_params=pltpu.CompilerParams(
            collective_id=0, has_side_effects=True, vmem_limit_bytes=VMEM_BYTES
        ),
        name="whole",
    )(
        cond[None], ctx_cond[None], mod_weight, latents, context, query_weight, key_matrix, value_matrix,
        query_gain[None], key_gain[None], cos, sin, out_weight, latents,
    )


def solution(mesh):
    placed = (
        P(("sp", "tp"), None),
        P("sp", None),
        P("sp"),
        P("sp"),
        P("sp", "tp"),
        P(None, "tp"),
        P(None, "tp"),
        P(None, "tp"),
        P("tp", None),
        P(),
        P(),
    )
    return jax.shard_map(
        body, mesh=mesh, in_specs=placed, out_specs=P(("sp", "tp"), None), check_vma=False
    )
```
